32 devices in a mesh: sp: 8 (over z, x), tp: 4 (over y, core).
Axes of the slice: x: 2, y: 2, z: 4, core: 2. Of those that a mesh axis runs over, the one named last changes fastest.
Arguments:
- query_proj: bfloat16 [4096, 1024], P('sp', 'tp'), may hold values from -6 to 6
- projected_keys: bfloat16 [4096, 512], P('sp', 'tp'), may hold values from -6 to 6
- projected_values: bfloat16 [4096, 512], P('sp', 'tp'), may hold values from -6 to 6
- residual: bfloat16 [4096, 2048], P(('sp', 'tp')), may hold values from -6 to 6
- out_weight: bfloat16 [1024, 2048], replicated, may hold values from -0.1875 to 0.1875
- mix_gain: float32 [2048], replicated, may hold values from 0.1 to 1.9
- norm_gain: float32 [2048], replicated, may hold values from 0.1 to 1.9
- route_expert: int32 [4096, 2], P(('sp', 'tp')), may hold values from 0 to 31, all different within a row; in each aligned block of 128 rows (0 to 127, 128 to 255, ...) at most 16 rows name the same one
- route_weight: float32 [4096, 2], P(('sp', 'tp')), may hold values from 0.2 to 1
- expert_gate: bfloat16 [32, 2048, 1024], P(('sp', 'tp')), may hold values from -0.125 to 0.125
- expert_up: bfloat16 [32, 2048, 1024], P(('sp', 'tp')), may hold values from -0.125 to 0.125
- expert_down: bfloat16 [32, 1024, 2048], P(('sp', 'tp')), may hold values from -0.1875 to 0.1875
Outputs:
- output: bfloat16 [4096, 2048], P(('sp', 'tp'))
The draws below stay inside these ranges and needn't reach their ends.
Inputs may be any that keep to these rules, and one draw needn't show every extreme that they name: `route_expert`: each row names 2 different experts. The rows of one device (aligned blocks of 128 rows) name any one expert at most 16 times, and in some blocks some expert is named exactly 16 times.
All inputs are finite; a program needn't handle non-finite values.
Results may differ from the reference program's by a relative error of at most 0.015.
Values may be sent and summed in bfloat16 or wider, within the bound.
A program may use at most 128 MiB of HBM per device.

```python
import math
import jax
import jax.numpy as jnp
import numpy as np
from jax import lax

D = 2048
QUERY_HEADS = 16
KEY_VALUE_HEADS = 8
HEAD_SIZE = 64
FF = 1024
TOP = 2
GRID_W = 64
ROWS = 128
SEQUENCE_TOKENS = 4096
EXPERTS = 32
CAP = 16
N_SP = 8
N_TP = 4


def block_levels(own_key, shape, cuts, low, top_value):
    def one(dim, shards_of):
        heights = jax.random.uniform(jax.random.fold_in(jax.random.fold_in(own_key, 6), dim), (shards_of,), jnp.float32, low / len(cuts), top_value / len(cuts))
        return jnp.repeat(jnp.exp(heights), shape[dim] // shards_of).reshape((-1,) + (1,) * (len(shape) - dim - 1))

    gain = one(*cuts[0])
    for cut in cuts[1:]:
        gain = gain * one(*cut)
    return gain


def deal_out(key, own, number, rows, count, top, bound, skew):
    ranking = jax.random.permutation(key, count)
    heavy_load, common = shares(count, rows * top, bound, skew, True), shares(count, rows * top, bound, skew, False)
    places = jnp.arange(count)

    def named(lengths, rotation):
        used = int((lengths > 0).sum())
        fixed = max(1, used // 4)
        moved = fixed + (places - fixed + rotation * (used - fixed)) % max(1, count - fixed)
        return jnp.zeros((count,), jnp.int32).at[ranking[jnp.where(places < fixed, places, moved)]].set(jnp.asarray(lengths, jnp.int32))

    lengths = jnp.where(number % 4 == 0, named(heavy_load, number // 4), named(common, number - number // 4 - 1))
    mixed = jax.random.permutation(jax.random.fold_in(own, 3), count)
    source_of, taker = mixed[0:count // 2 * 2:2], mixed[1:count // 2 * 2:2]
    margin = jnp.minimum(lengths[source_of] - 1, bound - lengths[taker]) // 2
    margin = jnp.where((source_of == ranking[0]) | (taker == ranking[0]) | (lengths[taker] == 0), 0, jnp.maximum(margin, 0))
    moved = jax.random.randint(jax.random.fold_in(own, 4), (count // 2,), 0, 1 << 20) % (margin + 1)
    lengths = lengths.at[source_of].add(-moved).at[taker].add(moved)
    labels = jnp.searchsorted(jnp.cumsum(lengths), jnp.arange(rows * top), side="right").astype(jnp.int32)
    grid = labels.reshape(top, rows).T
    grid = grid[jax.random.permutation(jax.random.fold_in(own, 1), rows)]
    rotation = jax.random.randint(jax.random.fold_in(own, 2), (rows, 1), 0, top)
    return jnp.take_along_axis(grid, (jnp.arange(top)[None, :] + rotation) % top, axis=1)


def shares(amount, total, reach, slope, full):
    weights = [(1 << 20) // math.isqrt(grade ** slope) + 1 for grade in range(1, amount + 1)]
    largest = reach if full else min(reach, max(-(-total // amount), total * weights[0] // sum(weights)))
    least = 1 if total - largest >= amount - 1 else 0
    given, spare = [largest] + [least] * (amount - 1), total - largest - least * (amount - 1)
    while spare > 0:
        candidates = [i for i in range(1, amount) if given[i] < largest] or [i for i in range(1, amount) if given[i] < reach]
        pool, budget = sum([weights[i] for i in candidates]), spare
        for i in candidates:
            more = min(reach - given[i], max(1, budget * weights[i] // pool), spare)
            given[i] = given[i] + more
            spare = spare - more
    return np.array(given)


def bell_draw(rng, dims, deviation, most, pieces=(), kind=jnp.bfloat16):
    entries = jax.random.normal(rng, dims, jnp.float32) * deviation
    if len(pieces) > 0:
        entries = block_levels(rng, dims, pieces, -0.22, 0.18) * entries
    return jnp.clip(entries, min=-most, max=most).astype(kind)


def setup_inputs(seed: int = 0) -> dict:
    key_list = jax.random.split(jax.random.key(seed), 13)
    query_proj = bell_draw(key_list[0], (SEQUENCE_TOKENS, QUERY_HEADS * HEAD_SIZE), 1.0, 6.0, ((0, 8), (1, 4)))
    projected_keys = bell_draw(key_list[1], (SEQUENCE_TOKENS, KEY_VALUE_HEADS * HEAD_SIZE), 1.0, 6.0, ((0, 8), (1, 4)))
    projected_values = bell_draw(key_list[2], (SEQUENCE_TOKENS, KEY_VALUE_HEADS * HEAD_SIZE), 1.0, 6.0, ((0, 8), (1, 4)))
    residual = bell_draw(key_list[3], (SEQUENCE_TOKENS, D), 1.0, 6.0, ((0, 32),))
    out_weight = bell_draw(key_list[4], (QUERY_HEADS * HEAD_SIZE, D), (QUERY_HEADS * HEAD_SIZE) ** -0.5, 0.1875)
    mix_gain = jnp.clip(1.0 + 0.18 * jax.random.normal(key_list[5], (D,), jnp.float32), 0.1, 1.9)
    norm_gain = jnp.clip(1.0 + 0.18 * jax.random.normal(key_list[6], (D,), jnp.float32), 0.1, 1.9)
    route_expert_keys = jax.random.split(jax.random.fold_in(key_list[7], 1), SEQUENCE_TOKENS // ROWS)
    route_expert_turns = jax.random.permutation(jax.random.fold_in(key_list[7], 3), SEQUENCE_TOKENS // ROWS)
    route_expert = jax.vmap(lambda own, number: deal_out(jax.random.fold_in(key_list[7], 2), own, number, ROWS, EXPERTS, TOP, CAP, 2))(route_expert_keys, route_expert_turns).reshape((SEQUENCE_TOKENS, TOP))
    route_weight = jnp.clip(0.2 + 0.8 * jax.random.uniform(key_list[8], (SEQUENCE_TOKENS, TOP), jnp.float32) ** block_levels(key_list[8], (SEQUENCE_TOKENS, TOP), ((0, 32),), -0.2, 0.2), 0.2, 1.0)
    expert_gate = bell_draw(key_list[9], (EXPERTS, D, FF), D ** -0.5, 0.125, ((0, 32),))
    expert_up = bell_draw(key_list[10], (EXPERTS, D, FF), D ** -0.5, 0.125, ((0, 32),))
    expert_down = bell_draw(key_list[11], (EXPERTS, FF, D), FF ** -0.5, 0.1875, ((0, 32),))
    return dict(query_proj=query_proj, projected_keys=projected_keys, projected_values=projected_values, residual=residual, out_weight=out_weight, mix_gain=mix_gain, norm_gain=norm_gain, route_expert=route_expert, route_weight=route_weight, expert_gate=expert_gate, expert_up=expert_up, expert_down=expert_down)


epsilon = 1e-06
base_theta = 10000.0

def unit_length_rows(values):
    values = values.astype(jnp.float32)
    return values * lax.rsqrt(lax.optimization_barrier(jnp.mean(values * values, axis=-1, keepdims=True)) + epsilon)

def rotary_embed(head_vecs, offset):
    row_count = head_vecs.shape[0]
    quarter = head_vecs.shape[-1] // 4
    places = offset + jnp.arange(row_count, dtype=jnp.int32)
    grid_row = (places // GRID_W).astype(jnp.float32)
    grid_col = (places % GRID_W).astype(jnp.float32)
    frequency = base_theta ** (-jnp.arange(quarter, dtype=jnp.float32) / quarter)
    row_angle = grid_row[:, None, None] * frequency
    col_angle = grid_col[:, None, None] * frequency
    row_cos, row_sin = (jnp.cos(row_angle), jnp.sin(row_angle))
    col_cos, col_sin = (jnp.cos(col_angle), jnp.sin(col_angle))
    row_first = head_vecs[..., :quarter]
    row_second = head_vecs[..., quarter:2 * quarter]
    col_first = head_vecs[..., 2 * quarter:3 * quarter]
    col_second = head_vecs[..., 3 * quarter:]
    return jnp.concatenate([row_first * row_cos - row_second * row_sin, row_second * row_cos + row_first * row_sin, col_first * col_cos - col_second * col_sin, col_second * col_cos + col_first * col_sin], axis=-1)

def reference(query_proj, projected_keys, projected_values, residual, out_weight, mix_gain, norm_gain, route_expert, route_weight, expert_gate, expert_up, expert_down):
    query_group = QUERY_HEADS // KEY_VALUE_HEADS
    query_prepared = rotary_embed(unit_length_rows(query_proj.reshape(SEQUENCE_TOKENS, QUERY_HEADS, HEAD_SIZE)), 0).astype(jnp.bfloat16)
    query_prepared = query_prepared.reshape(SEQUENCE_TOKENS, KEY_VALUE_HEADS, query_group, HEAD_SIZE)
    key_prepared = rotary_embed(unit_length_rows(projected_keys.reshape(SEQUENCE_TOKENS, KEY_VALUE_HEADS, HEAD_SIZE)), 0).astype(jnp.bfloat16)
    k_wide = key_prepared.astype(jnp.float32)
    value_broad = projected_values.reshape(SEQUENCE_TOKENS, KEY_VALUE_HEADS, HEAD_SIZE).astype(jnp.float32)
    scale = HEAD_SIZE ** (-0.5)
    model_width = math.gcd(SEQUENCE_TOKENS, 256)

    def attend(q_block):
        scores = jnp.einsum('thgd,nhd->thgn', q_block.astype(jnp.float32), k_wide) * scale
        weights = jnp.exp(scores)
        totals = lax.optimization_barrier(jnp.sum(weights, axis=-1))
        weights_low = lax.optimization_barrier(weights.astype(jnp.bfloat16))
        sums = jnp.einsum('thgn,nhd->thgd', weights_low.astype(jnp.float32), value_broad)
        return (sums / totals[..., None]).astype(jnp.bfloat16)
    block_list = query_prepared.reshape(SEQUENCE_TOKENS // model_width, model_width, KEY_VALUE_HEADS, query_group, HEAD_SIZE)
    attended = lax.map(attend, block_list).reshape(SEQUENCE_TOKENS, QUERY_HEADS * HEAD_SIZE)
    mixed = jnp.dot(attended, out_weight, preferred_element_type=jnp.float32)
    stream = (residual.astype(jnp.float32) + unit_length_rows(mixed) * mix_gain).astype(jnp.bfloat16)
    normed = (unit_length_rows(stream) * norm_gain).astype(jnp.bfloat16)
    limit = N_SP * N_TP * CAP
    flat_expert = route_expert.reshape(-1).astype(jnp.int32)
    order = jnp.argsort(flat_expert, stable=True).astype(jnp.int32)
    counts = lax.optimization_barrier(jnp.sum((flat_expert[:, None] == jnp.arange(EXPERTS, dtype=jnp.int32)[None, :]).astype(jnp.int32), axis=0))
    starts = (jnp.cumsum(counts) - counts).astype(jnp.int32)
    padded = jnp.concatenate([order, jnp.zeros((limit,), jnp.int32)])

    def one_expert(index):
        chosen = lax.dynamic_slice_in_dim(padded, starts[index], limit)
        rows_in = normed[chosen // TOP]
        gate_pre = jnp.dot(rows_in, expert_gate[index], preferred_element_type=jnp.float32)
        up_pre = jnp.dot(rows_in, expert_up[index], preferred_element_type=jnp.float32)
        expert_act = (jax.nn.silu(gate_pre) * up_pre).astype(jnp.bfloat16)
        return jnp.dot(expert_act, expert_down[index], preferred_element_type=jnp.float32).astype(jnp.bfloat16)
    results = lax.map(one_expert, jnp.arange(EXPERTS, dtype=jnp.int32))
    position = jnp.argsort(order, stable=True).astype(jnp.int32)
    rank = (position - starts[flat_expert]).astype(jnp.int32)
    picked = results[flat_expert, rank].reshape(SEQUENCE_TOKENS, TOP, D)
    combined = lax.optimization_barrier(jnp.sum(picked.astype(jnp.float32) * route_weight[:, :, None], axis=1))
    return (stream.astype(jnp.float32) + combined).astype(jnp.bfloat16)
```

```python
import functools
import math

import jax
import jax.numpy as jnp
from jax import lax
from jax.experimental import pallas as pl
from jax.experimental.pallas import tpu as pltpu
from jax.sharding import PartitionSpec as P

D = 2048
HEAD_SIZE = 64
GRID_W = 64


epsilon = 1e-06
base_theta = 10000.0


def unit_length_rows(values):
    values = values.astype(jnp.float32)
    return values * lax.rsqrt(jnp.mean(values * values, axis=-1, keepdims=True) + epsilon)


MESH = pl.DeviceIdType.MESH
LANES = 2 * HEAD_SIZE


def ring_step(sp, delta, n, nz, nx):
    z, x = sp // nx, sp % nx
    place = x * nz + z + (x % 2) * (nz - 1 - 2 * z)
    place = (place + delta + n) % n
    x = place // nz
    z = place % nz
    z = z + (x % 2) * (nz - 1 - 2 * z)
    return z * nx + x


def attend_kernel(
    n, nz, nx, ntp, group,
    q_ref, k_ref, v_ref, cos_ref, sin_ref, swap_ref, ones_ref,
    out_ref,
    qs, acc, fb, bb, att, rx,
    send_f, recv_f, send_b, recv_b, send_t, recv_t,
):
    sp = lax.axis_index("sp")
    tp = lax.axis_index("tp")
    toks = q_ref.shape[0]
    heads = q_ref.shape[1] // HEAD_SIZE
    half = toks // 2
    steps = n - 1
    nxt = ring_step(sp, 1, n, nz, nx)
    prv = ring_step(sp, -1, n, nz, nx)

    barrier = pltpu.get_barrier_semaphore()
    for other in (nxt, prv):
        pl.semaphore_signal(barrier, inc=1, device_id=(other, tp), device_id_type=MESH)
    for d in range(1, ntp):
        pl.semaphore_signal(
            barrier, inc=1, device_id=(sp, (tp + d) % ntp), device_id_type=MESH
        )

    cos = cos_ref[...]
    sin = sin_ref[...]
    low = lax.broadcasted_iota(jnp.int32, (toks, LANES), 1) < HEAD_SIZE

    def prepare(block):
        wide = block.astype(jnp.float32)
        square = wide * wide
        hi = square.astype(jnp.bfloat16)
        lo = (square - hi.astype(jnp.float32)).astype(jnp.bfloat16)
        mean = jnp.dot(hi, ones_ref[...], preferred_element_type=jnp.float32) + jnp.dot(
            lo, ones_ref[...], preferred_element_type=jnp.float32
        )
        partner = jnp.dot(block, swap_ref[...], preferred_element_type=jnp.float32)
        return (wide * cos + partner * sin) * lax.rsqrt(mean + epsilon)

    keys = prepare(k_ref[...]).astype(jnp.bfloat16)
    vals = v_ref[...]
    for c in range(2):
        rows = slice(c * half, (c + 1) * half)
        fb[c, 0] = keys[rows]
        fb[c, 1] = vals[rows]
        bb[1 - c, 0] = keys[rows]
        bb[1 - c, 1] = vals[rows]

    def forward(i):
        return pltpu.make_async_remote_copy(
            src_ref=fb.at[i], dst_ref=fb.at[i + 2],
            send_sem=send_f.at[i], recv_sem=recv_f.at[i],
            device_id=(nxt, tp), device_id_type=MESH,
        )

    def backward(i):
        return pltpu.make_async_remote_copy(
            src_ref=bb.at[i], dst_ref=bb.at[i + 2],
            send_sem=send_b.at[i], recv_sem=recv_b.at[i],
            device_id=(prv, tp), device_id_type=MESH,
        )

    pl.semaphore_wait(barrier, 2 + ntp - 1)
    for i in range(2):
        forward(i).start()
        backward(i).start()

    scale = HEAD_SIZE ** (-0.5)
    for t in range(heads // 2):
        ready = prepare(q_ref[:, t * LANES : (t + 1) * LANES]) * scale
        for h in (2 * t, 2 * t + 1):
            side = (h // group) % 2
            lined = ready if h % 2 == side else pltpu.roll(ready, HEAD_SIZE, 1)
            keep = low if side == 0 else jnp.logical_not(low)
            qs[h * toks : (h + 1) * toks] = jnp.where(keep, lined, 0.0).astype(jnp.bfloat16)
    acc[...] = jnp.zeros_like(acc)
    tile = math.gcd(toks, 256)
    vlow = lax.broadcasted_iota(jnp.int32, (toks, LANES), 1) < HEAD_SIZE

    def one_step(j, carry):
        at = j + jnp.minimum(j, 1)

        @pl.when(j > 0)
        def _():
            forward(j - 1).wait_recv()
            backward(j - 1).wait_recv()

        @pl.when(jnp.logical_and(j > 0, j + 1 < steps))
        def _():
            forward(j + 1).start()
            backward(j + 1).start()

        kk = jnp.concatenate([fb[at, 0], bb[at, 0]], axis=0)
        vv = jnp.concatenate([fb[at, 1], bb[at, 1]], axis=0).astype(jnp.float32)
        sided = (
            jnp.where(vlow, vv, 1.0).astype(jnp.bfloat16),
            jnp.where(vlow, 1.0, vv).astype(jnp.bfloat16),
        )
        for h in range(heads):
            for r in range(toks // tile):
                rows = slice(h * toks + r * tile, h * toks + (r + 1) * tile)
                scores = lax.dot_general(
                    qs[rows], kk, (((1,), (1,)), ((), ())),
                    preferred_element_type=jnp.float32,
                )
                weights = jnp.exp(scores).astype(jnp.bfloat16)
                acc[rows] += jnp.dot(
                    weights, sided[(h // group) % 2], preferred_element_type=jnp.float32
                )
        return carry

    lax.fori_loop(0, steps + 1, one_step, 0)

    share = toks // ntp
    for t in range(heads // 2):
        parts = []
        for h in (2 * t, 2 * t + 1):
            mine = acc[h * toks : (h + 1) * toks]
            turned = pltpu.roll(mine, HEAD_SIZE, 1)
            parts.append(mine / turned if h % 2 == (h // group) % 2 else turned / mine)
        done = jnp.where(low, parts[0], parts[1]).astype(jnp.bfloat16)
        for p in range(ntp):
            att[p, :, t * LANES : (t + 1) * LANES] = done[p * share : (p + 1) * share]

    def across(d):
        to = (tp + d) % ntp
        return pltpu.make_async_remote_copy(
            src_ref=att.at[to], dst_ref=rx.at[tp],
            send_sem=send_t.at[d], recv_sem=recv_t.at[d],
            device_id=(sp, to), device_id_type=MESH,
        )

    for d in range(1, ntp):
        across(d).start()
    rx[tp] = att[tp]
    for i in range(steps):
        forward(i).wait_send()
        backward(i).wait_send()
    for d in range(1, ntp):
        across(d).wait_recv()
    width = q_ref.shape[1]
    for p in range(ntp):
        out_ref[:, p * width : (p + 1) * width] = rx[p]
    for d in range(1, ntp):
        across(d).wait_send()


def ring_sizes(mesh, n):
    try:
        coords = [tuple(d.coords) for d in mesh.devices[:, 0]]
        nz = len({c[2] for c in coords})
        nx = len({c[0] for c in coords})
        if nz * nx == n and nz > 1:
            return nz, nx
    except Exception:
        pass
    return n, 1


def attend(mesh, query_proj, projected_keys, projected_values):
    n, ntp = mesh.shape["sp"], mesh.shape["tp"]
    nz, nx = ring_sizes(mesh, n)
    toks, width = query_proj.shape
    heads = width // HEAD_SIZE
    group = heads // (projected_keys.shape[1] // HEAD_SIZE)
    spare = LANES - projected_keys.shape[1]
    if spare:
        projected_keys = jnp.pad(projected_keys, ((0, 0), (0, spare)))
        projected_values = jnp.pad(projected_values, ((0, 0), (0, spare)))
    quarter = HEAD_SIZE // 4
    places = lax.axis_index("sp") * toks + jnp.arange(toks, dtype=jnp.int32)
    frequency = base_theta ** (-jnp.arange(quarter, dtype=jnp.float32) / quarter)
    lane = jnp.arange(LANES, dtype=jnp.int32)
    on_row = (lane % HEAD_SIZE) < 2 * quarter
    spot = jnp.where(on_row[None, :], (places // GRID_W)[:, None], (places % GRID_W)[:, None])
    angle = spot.astype(jnp.float32) * jnp.tile(frequency, LANES // quarter)[None, :]
    first = (lane // quarter) % 2 == 0
    source = jnp.where(first, lane + quarter, lane - quarter)
    swap = jnp.where(
        lane[:, None] == source[None, :], jnp.where(first, -1.0, 1.0)[None, :], 0.0
    ).astype(jnp.bfloat16)
    ones = jnp.where(
        lane[:, None] // HEAD_SIZE == lane[None, :] // HEAD_SIZE, 1.0 / HEAD_SIZE, 0.0
    ).astype(jnp.bfloat16)
    share = toks // ntp
    dma = pltpu.SemaphoreType.DMA
    return pl.pallas_call(
        functools.partial(attend_kernel, n, nz, nx, ntp, group),
        out_shape=jax.ShapeDtypeStruct((share, ntp * width), jnp.bfloat16),
        in_specs=[pl.BlockSpec(memory_space=pltpu.VMEM)] * 7,
        out_specs=pl.BlockSpec(memory_space=pltpu.VMEM),
        scratch_shapes=[
            pltpu.VMEM((heads * toks, LANES), jnp.bfloat16),
            pltpu.VMEM((heads * toks, LANES), jnp.float32),
            pltpu.VMEM((n + 1, 2, toks // 2, LANES), jnp.bfloat16),
            pltpu.VMEM((n + 1, 2, toks // 2, LANES), jnp.bfloat16),
            pltpu.VMEM((ntp, share, width), jnp.bfloat16),
            pltpu.VMEM((ntp, share, width), jnp.bfloat16),
            dma((n - 1,)), dma((n - 1,)), dma((n - 1,)), dma((n - 1,)),
            dma((ntp,)), dma((ntp,)),
        ],
        compiler_params=pltpu.CompilerParams(
            collective_id=0, has_side_effects=True, vmem_limit_bytes=40 << 20
        ),
        name="attend",
    )(query_proj, projected_keys, projected_values, jnp.cos(angle), jnp.sin(angle), swap, ones)


def moe_kernel(
    nz, nx, ntp, cap, cuts,
    normed, stream, route, share_w, gate_hbm, up_hbm, down_hbm,
    out_ref,
    info, blk, tx, rx, res, ret, inc, part, snd, place, weigh, act, gate, up, down,
    send_i, recv_i, send_u, send_d, recv_z, send_o, recv_o, send_r, recv_r, send_p, recv_p, wsem,
):
    sp = lax.axis_index("sp")
    tp = lax.axis_index("tp")
    z = sp // nx
    p = (sp % nx) * ntp + tp
    plane = nx * ntp
    slots = plane * cap
    toks, width = normed.shape
    wide = width // cuts
    others = (plane - 1) * cap

    def device(zz, pp):
        return (zz * nx + pp // ntp, pp % ntp)

    def cols(c):
        return pl.ds(pl.multiple_of(c * wide, wide), wide)

    def rows(pp):
        return pl.ds(pl.multiple_of(pp * cap, cap), cap)

    def remote(src, dst, send, recv, to):
        return pltpu.make_async_remote_copy(
            src_ref=src, dst_ref=dst, send_sem=send, recv_sem=recv,
            device_id=to, device_id_type=MESH,
        )

    def loop(first, last, action):
        def body(i, carry):
            action(i)
            return carry

        lax.fori_loop(first, last, body, 0)

    def facts(k):
        to = (z + k) % nz
        return remote(info.at[z], info.at[z], send_i.at[k], recv_i.at[k], device(to, p))

    def facts_in(k):
        zz = (z - k + nz) % nz
        return remote(info.at[zz], info.at[zz], send_i.at[k], recv_i.at[k], device(zz, p))

    def own_hop(c, up_way):
        send = send_u if up_way else send_d
        return remote(
            normed.at[:, cols(c)], blk.at[z, :, cols(c)], send.at[z, c], recv_z.at[z, c],
            device(z + 1 if up_way else z - 1, p),
        )

    def hop(zz, c, up_way):
        send = send_u if up_way else send_d
        return remote(
            blk.at[zz, :, cols(c)], blk.at[zz, :, cols(c)], send.at[zz, c], recv_z.at[zz, c],
            device(z + 1 if up_way else z - 1, p),
        )

    def dispatch(zz, c, q):
        pp = (p + q) % plane
        return remote(
            tx.at[zz, rows(pp), cols(c)], rx.at[zz, rows(p), cols(c)],
            send_o.at[zz], recv_o.at[zz], device(z, pp),
        )

    def dispatch_all(zz):
        some = pl.ds(0, others)
        return remote(tx.at[zz, some], rx.at[zz, some], send_o.at[zz], recv_o.at[zz], device(z, p))

    def answer(zz, c, q):
        pp = (p + q) % plane
        return remote(
            res.at[zz, rows(pp), cols(c)], ret.at[zz, rows(p), cols(c)],
            send_r.at[zz], recv_r.at[zz, c], device(z, pp),
        )

    def answer_in(zz, c):
        some = pl.ds(0, others)
        return remote(
            res.at[zz, some, cols(c)], ret.at[zz, some, cols(c)],
            send_r.at[zz], recv_r.at[zz, c], device(z, p),
        )

    def answer_sent(zz):
        some = pl.ds(0, others)
        return remote(res.at[zz, some], ret.at[zz, some], send_r.at[zz], recv_r.at[zz, 0], device(z, p))

    def partial_out(zz, c):
        step = jnp.where(zz > z, 1, -1)
        slot = jnp.where(zz == z + 1, nz, zz)
        return remote(
            snd.at[zz, :, cols(c)], inc.at[slot, :, cols(c)],
            send_p.at[zz, c], recv_p.at[slot, c], device(z + step, p),
        )

    def partial_in(slot, c):
        return remote(
            snd.at[0, :, cols(c)], inc.at[slot, :, cols(c)],
            send_p.at[0, c], recv_p.at[slot, c], device(z, p),
        )

    barrier = pltpu.get_barrier_semaphore()
    for k in range(1, nz):
        pl.semaphore_signal(barrier, inc=1, device_id=device((z + k) % nz, p), device_id_type=MESH)
    for q in range(1, plane):
        pl.semaphore_signal(barrier, inc=1, device_id=device(z, (p + q) % plane), device_id_type=MESH)
    loads = [
        pltpu.make_async_copy(gate_hbm.at[0], gate, wsem.at[0]),
        pltpu.make_async_copy(up_hbm.at[0], up, wsem.at[1]),
        pltpu.make_async_copy(down_hbm.at[0], down, wsem.at[2]),
    ]
    for load in loads:
        load.start()

    experts = nz * plane
    at_expert = lax.broadcasted_iota(jnp.int32, (experts, toks), 0)
    named = [at_expert == route[k : k + 1, :] for k in range(2)]
    count = (named[0].astype(jnp.float32) + named[1].astype(jnp.float32)).astype(jnp.bfloat16)
    before = (
        lax.broadcasted_iota(jnp.int32, (toks, toks), 0)
        < lax.broadcasted_iota(jnp.int32, (toks, toks), 1)
    ).astype(jnp.float32).astype(jnp.bfloat16)
    earlier = jnp.dot(count, before, preferred_element_type=jnp.float32)
    lines = []
    for k in range(2):
        rank = jnp.sum(jnp.where(named[k], earlier, 0.0), axis=0, keepdims=True)
        lines.append(route[k : k + 1, :].astype(jnp.float32) * float(cap) + rank)
    info[z] = jnp.concatenate(
        lines + [share_w[...], jnp.zeros((4, toks), jnp.float32)], axis=0
    )

    pl.semaphore_wait(barrier, nz - 1 + plane - 1)
    for k in range(1, nz):
        facts(k).start()

    @pl.when(z + 1 < nz)
    def _():
        loop(0, cuts, lambda c: own_hop(c, True).start())

    @pl.when(z > 0)
    def _():
        loop(0, cuts, lambda c: own_hop(c, False).start())

    def learn(zz):
        known = info[zz]
        spot = (
            lax.broadcasted_iota(jnp.int32, (slots, toks), 0) + z * slots
        ).astype(jnp.float32)
        first = spot == known[0:1, :]
        second = spot == known[1:2, :]
        place[zz] = jnp.where(first | second, 1.0, 0.0).astype(jnp.bfloat16)
        amount = jnp.where(first, known[2:3, :], 0.0) + jnp.where(second, known[3:4, :], 0.0)
        turned = amount.T
        hi = turned.astype(jnp.bfloat16)
        weigh[zz, :, 0:slots] = hi
        weigh[zz, :, slots : 2 * slots] = (turned - hi.astype(jnp.float32)).astype(jnp.bfloat16)

    def pack(zz, c, block):
        packed = jnp.dot(
            place[zz], block, preferred_element_type=jnp.float32
        ).astype(jnp.bfloat16)
        tx[zz, :, cols(c)] = packed
        for q in range(1, plane):
            dispatch(zz, c, q).start()
        rx[zz, rows(p), cols(c)] = tx[zz, rows(p), cols(c)]

    def columns(first, total, body):
        tile = math.gcd(total, 256)

        def one(c, carry):
            body(pl.ds(pl.multiple_of(first + c * tile, tile), tile))
            return carry

        lax.fori_loop(0, total // tile, one, 0)

    def expert(zz):
        dispatch_all(zz).wait_recv()

        def hidden(at):
            taken = rx[zz]
            pre = jnp.dot(taken, gate[:, at], preferred_element_type=jnp.float32)
            lift = jnp.dot(taken, up[:, at], preferred_element_type=jnp.float32)
            act[:, at] = (pre / (1.0 + jnp.exp(-pre)) * lift).astype(jnp.bfloat16)

        def project(at):
            res[zz, :, at] = jnp.dot(
                act[...], down[:, at], preferred_element_type=jnp.float32
            ).astype(jnp.bfloat16)

        columns(0, gate.shape[1], hidden)

        def send(c):
            columns(c * wide, wide, project)
            for q in range(1, plane):
                answer(zz, c, q).start()
            ret[zz, rows(p), cols(c)] = res[zz, rows(p), cols(c)]

        loop(0, cuts, send)

    def gather(zz):
        last = jnp.logical_and(
            zz != z,
            jnp.logical_or(
                jnp.logical_and(zz > z, z == 0), jnp.logical_and(zz < z, z == nz - 1)
            ),
        )

        def one(c):
            answer_in(zz, c).wait_recv()
            back = ret[zz, :, cols(c)]
            total = jnp.dot(
                weigh[zz, :, 0:slots], back, preferred_element_type=jnp.float32
            ) + jnp.dot(
                weigh[zz, :, slots : 2 * slots], back, preferred_element_type=jnp.float32
            )
            part[zz, :, cols(c)] = total

            @pl.when(last)
            def _():
                snd[zz, :, cols(c)] = total.astype(jnp.bfloat16)
                partial_out(zz, c).start()

        loop(0, cuts, one)

    def both(d, action):
        def side(s, carry):
            zz = z + d * (2 * s - 1)
            valid = jnp.logical_and(jnp.logical_and(zz >= 0, zz < nz), jnp.logical_or(d > 0, s == 0))

            @pl.when(valid)
            def _():
                action(zz, s)

            return carry

        lax.fori_loop(0, 2, side, 0)

    def receive(d, c):
        def forward(zz, s):
            hop(zz, c, True).wait_recv()

            @pl.when(jnp.logical_and(zz < z, z + 1 < nz))
            def _():
                hop(zz, c, True).start()

            @pl.when(jnp.logical_and(zz > z, z > 0))
            def _():
                hop(zz, c, False).start()

        both(d, forward)
        both(d, lambda zz, s: pack(zz, c, blk[zz, :, cols(c)]))

    learn(z)
    loop(0, cuts, lambda c: pack(z, c, normed[:, cols(c)]))
    for k in range(1, nz):
        facts_in(k).wait_recv()
        learn((z - k + nz) % nz)
    for load in loads:
        load.wait()

    def turn(d, carry):
        @pl.when(d < nz)
        def _():
            receive(d, 0)

        both(d - 1, lambda zz, s: expert(zz))

        @pl.when(d < nz)
        def _():
            loop(1, cuts, lambda c: receive(d, c))

        both(d - 1, lambda zz, s: gather(zz))
        return carry

    lax.fori_loop(1, nz + 1, turn, 0)

    below = 2 * z < nz - 1

    def relay(level, c):
        def pass_on(s, carry):
            upward = jnp.where(below, s == 0, s == 1)
            zz = jnp.where(upward, level, nz - 1 - level)
            valid = jnp.where(
                upward, jnp.logical_and(zz > z, z > 0), jnp.logical_and(zz < z, z < nz - 1)
            )

            @pl.when(valid)
            def _():
                partial_in(zz, c).wait_recv()
                snd[zz, :, cols(c)] = (
                    part[zz, :, cols(c)] + inc[zz, :, cols(c)].astype(jnp.float32)
                ).astype(jnp.bfloat16)
                partial_out(zz, c).start()

            return carry

        lax.fori_loop(0, 2, pass_on, 0)

    loop(1, nz, lambda level: loop(0, cuts, lambda c: relay(level, c)))

    def finish(c):
        @pl.when(z > 0)
        def _():
            partial_in(nz, c).wait_recv()
            part[z, :, cols(c)] += inc[nz, :, cols(c)].astype(jnp.float32)

        @pl.when(z + 1 < nz)
        def _():
            partial_in(z, c).wait_recv()
            part[z, :, cols(c)] += inc[z, :, cols(c)].astype(jnp.float32)

        out_ref[:, cols(c)] = (
            stream[:, cols(c)].astype(jnp.float32) + part[z, :, cols(c)]
        ).astype(jnp.bfloat16)

    loop(0, cuts, finish)

    for k in range(1, nz):
        facts(k).wait_send()

    def sent(zz):
        dispatch_all(zz).wait_send()
        answer_sent(zz).wait_send()

        def one(c):
            @pl.when(jnp.logical_and(zz <= z, z + 1 < nz))
            def _():
                hop(zz, c, True).wait_send()

            @pl.when(jnp.logical_and(zz >= z, z > 0))
            def _():
                hop(zz, c, False).wait_send()

            @pl.when(zz != z)
            def _():
                partial_out(zz, c).wait_send()

        loop(0, cuts, one)

    loop(0, nz, sent)


def moe(mesh, nz, nx, cap, normed, stream, route, share_w, expert_gate, expert_up, expert_down):
    ntp = mesh.shape["tp"]
    plane = nx * ntp
    slots = plane * cap
    toks, width = normed.shape
    ff = expert_gate.shape[2]
    cuts = max(1, width // 512)
    dma = pltpu.SemaphoreType.DMA
    low = jnp.bfloat16
    return pl.pallas_call(
        functools.partial(moe_kernel, nz, nx, ntp, cap, cuts),
        out_shape=jax.ShapeDtypeStruct(stream.shape, low),
        in_specs=[pl.BlockSpec(memory_space=pltpu.VMEM)] * 4
        + [pl.BlockSpec(memory_space=pl.ANY)] * 3,
        out_specs=pl.BlockSpec(memory_space=pltpu.VMEM),
        scratch_shapes=[
            pltpu.VMEM((nz, 8, toks), jnp.float32),
            pltpu.VMEM((nz, toks, width), low),
            pltpu.VMEM((nz, slots, width), low),
            pltpu.VMEM((nz, slots, width), low),
            pltpu.VMEM((nz, slots, width), low),
            pltpu.VMEM((nz, slots, width), low),
            pltpu.VMEM((nz + 1, toks, width), low),
            pltpu.VMEM((nz, toks, width), jnp.float32),
            pltpu.VMEM((nz, toks, width), low),
            pltpu.VMEM((nz, slots, toks), low),
            pltpu.VMEM((nz, toks, 2 * slots), low),
            pltpu.VMEM((slots, ff), low),
            pltpu.VMEM((width, ff), low),
            pltpu.VMEM((width, ff), low),
            pltpu.VMEM((ff, width), low),
            dma((nz,)), dma((nz,)),
            dma((nz, cuts)), dma((nz, cuts)), dma((nz, cuts)),
            dma((nz,)), dma((nz,)),
            dma((nz,)), dma((nz, cuts)),
            dma((nz, cuts)), dma((nz + 1, cuts)),
            dma((3,)),
        ],
        compiler_params=pltpu.CompilerParams(
            collective_id=1, has_side_effects=True, vmem_limit_bytes=62 << 20
        ),
        name="moe",
    )(normed, stream, route, share_w, expert_gate, expert_up, expert_down)


def local(
    mesh,
    query_proj,
    projected_keys,
    projected_values,
    residual,
    out_weight,
    mix_gain,
    norm_gain,
    route_expert,
    route_weight,
    expert_gate,
    expert_up,
    expert_down,
):
    by_token = attend(mesh, query_proj, projected_keys, projected_values)
    mixed = jnp.dot(by_token, out_weight, preferred_element_type=jnp.float32)
    stream = (residual.astype(jnp.float32) + unit_length_rows(mixed) * mix_gain).astype(
        jnp.bfloat16
    )
    normed = (unit_length_rows(stream) * norm_gain).astype(jnp.bfloat16)
    row_count = normed.shape[0]
    top_count = route_expert.shape[1]
    n = mesh.shape["sp"]
    experts = n * mesh.shape["tp"]
    capacity = -(-max(2, 2 * top_count * row_count // experts) // 16) * 16
    nz, nx = ring_sizes(mesh, n)
    return moe(
        mesh, nz, nx, capacity, normed, stream, route_expert.T, route_weight.T,
        expert_gate, expert_up, expert_down,
    )


def solution(mesh):
    return jax.shard_map(
        functools.partial(local, mesh),
        mesh=mesh,
        in_specs=(
            P("sp", "tp"),
            P("sp", "tp"),
            P("sp", "tp"),
            P(("sp", "tp"), None),
            P(),
            P(),
            P(),
            P(("sp", "tp"), None),
            P(("sp", "tp"), None),
            P(("sp", "tp"), None, None),
            P(("sp", "tp"), None, None),
            P(("sp", "tp"), None, None),
        ),
        out_specs=P(("sp", "tp"), None),
        check_vma=False,
    )
```

```python
import functools
import math

import jax
import jax.numpy as jnp
from jax import lax
from jax.experimental import pallas as pl
from jax.experimental.pallas import tpu as pltpu
from jax.sharding import PartitionSpec as P

D = 2048
HEAD_SIZE = 64
GRID_W = 64


epsilon = 1e-06
base_theta = 10000.0


def unit_length_rows(values):
    values = values.astype(jnp.float32)
    return values * lax.rsqrt(jnp.mean(values * values, axis=-1, keepdims=True) + epsilon)


MESH = pl.DeviceIdType.MESH
LANES = 2 * HEAD_SIZE


def ring_step(sp, delta, n, nz, nx):
    z, x = sp // nx, sp % nx
    place = x * nz + z + (x % 2) * (nz - 1 - 2 * z)
    place = (place + delta + n) % n
    x = place // nz
    z = place % nz
    z = z + (x % 2) * (nz - 1 - 2 * z)
    return z * nx + x


def attend_kernel(
    n, nz, nx, ntp, group,
    q_ref, k_ref, v_ref, cos_ref, sin_ref, swap_ref, ones_ref,
    out_ref,
    qs, acc, fb, bb, att, rx,
    send_f, recv_f, send_b, recv_b, send_t, recv_t,
):
    sp = lax.axis_index("sp")
    tp = lax.axis_index("tp")
    toks = q_ref.shape[0]
    heads = q_ref.shape[1] // HEAD_SIZE
    half = toks // 2
    steps = n - 1
    nxt = ring_step(sp, 1, n, nz, nx)
    prv = ring_step(sp, -1, n, nz, nx)

    barrier = pltpu.get_barrier_semaphore()
    for other in (nxt, prv):
        pl.semaphore_signal(barrier, inc=1, device_id=(other, tp), device_id_type=MESH)
    for d in range(1, ntp):
        pl.semaphore_signal(
            barrier, inc=1, device_id=(sp, (tp + d) % ntp), device_id_type=MESH
        )

    cos = cos_ref[...]
    sin = sin_ref[...]
    low = lax.broadcasted_iota(jnp.int32, (toks, LANES), 1) < HEAD_SIZE

    def prepare(block):
        wide = block.astype(jnp.float32)
        square = wide * wide
        hi = square.astype(jnp.bfloat16)
        lo = (square - hi.astype(jnp.float32)).astype(jnp.bfloat16)
        mean = jnp.dot(hi, ones_ref[...], preferred_element_type=jnp.float32) + jnp.dot(
            lo, ones_ref[...], preferred_element_type=jnp.float32
        )
        partner = jnp.dot(block, swap_ref[...], preferred_element_type=jnp.float32)
        return (wide * cos + partner * sin) * lax.rsqrt(mean + epsilon)

    keys = prepare(k_ref[...]).astype(jnp.bfloat16)
    vals = v_ref[...]
    for c in range(2):
        rows = slice(c * half, (c + 1) * half)
        fb[c, 0] = keys[rows]
        fb[c, 1] = vals[rows]
        bb[1 - c, 0] = keys[rows]
        bb[1 - c, 1] = vals[rows]

    def forward(i):
        return pltpu.make_async_remote_copy(
            src_ref=fb.at[i], dst_ref=fb.at[i + 2],
            send_sem=send_f.at[i], recv_sem=recv_f.at[i],
            device_id=(nxt, tp), device_id_type=MESH,
        )

    def backward(i):
        return pltpu.make_async_remote_copy(
            src_ref=bb.at[i], dst_ref=bb.at[i + 2],
            send_sem=send_b.at[i], recv_sem=recv_b.at[i],
            device_id=(prv, tp), device_id_type=MESH,
        )

    pl.semaphore_wait(barrier, 2 + ntp - 1)
    for i in range(2):
        forward(i).start()
        backward(i).start()

    scale = HEAD_SIZE ** (-0.5)
    for t in range(heads // 2):
        ready = prepare(q_ref[:, t * LANES : (t + 1) * LANES]) * scale
        for h in (2 * t, 2 * t + 1):
            side = (h // group) % 2
            lined = ready if h % 2 == side else pltpu.roll(ready, HEAD_SIZE, 1)
            keep = low if side == 0 else jnp.logical_not(low)
            qs[h * toks : (h + 1) * toks] = jnp.where(keep, lined, 0.0).astype(jnp.bfloat16)
    acc[...] = jnp.zeros_like(acc)
    tile = math.gcd(toks, 256)
    vlow = lax.broadcasted_iota(jnp.int32, (toks, LANES), 1) < HEAD_SIZE

    def one_step(j, carry):
        at = j + jnp.minimum(j, 1)

        @pl.when(j > 0)
        def _():
            forward(j - 1).wait_recv()
            backward(j - 1).wait_recv()

        @pl.when(jnp.logical_and(j > 0, j + 1 < steps))
        def _():
            forward(j + 1).start()
            backward(j + 1).start()

        kk = jnp.concatenate([fb[at, 0], bb[at, 0]], axis=0)
        vv = jnp.concatenate([fb[at, 1], bb[at, 1]], axis=0).astype(jnp.float32)
        sided = (
            jnp.where(vlow, vv, 1.0).astype(jnp.bfloat16),
            jnp.where(vlow, 1.0, vv).astype(jnp.bfloat16),
        )
        for h in range(heads):
            for r in range(toks // tile):
                rows = slice(h * toks + r * tile, h * toks + (r + 1) * tile)
                scores = lax.dot_general(
                    qs[rows], kk, (((1,), (1,)), ((), ())),
                    preferred_element_type=jnp.float32,
                )
                weights = jnp.exp(scores).astype(jnp.bfloat16)
                acc[rows] += jnp.dot(
                    weights, sided[(h // group) % 2], preferred_element_type=jnp.float32
                )
        return carry

    lax.fori_loop(0, steps + 1, one_step, 0)

    share = toks // ntp
    for t in range(heads // 2):
        parts = []
        for h in (2 * t, 2 * t + 1):
            mine = acc[h * toks : (h + 1) * toks]
            turned = pltpu.roll(mine, HEAD_SIZE, 1)
            parts.append(mine / turned if h % 2 == (h // group) % 2 else turned / mine)
        done = jnp.where(low, parts[0], parts[1]).astype(jnp.bfloat16)
        for p in range(ntp):
            att[p, :, t * LANES : (t + 1) * LANES] = done[p * share : (p + 1) * share]

    def across(d):
        to = (tp + d) % ntp
        return pltpu.make_async_remote_copy(
            src_ref=att.at[to], dst_ref=rx.at[tp],
            send_sem=send_t.at[d], recv_sem=recv_t.at[d],
            device_id=(sp, to), device_id_type=MESH,
        )

    for d in range(1, ntp):
        across(d).start()
    rx[tp] = att[tp]
    for i in range(steps):
        forward(i).wait_send()
        backward(i).wait_send()
    for d in range(1, ntp):
        across(d).wait_recv()
    width = q_ref.shape[1]
    for p in range(ntp):
        out_ref[:, p * width : (p + 1) * width] = rx[p]
    for d in range(1, ntp):
        across(d).wait_send()


def ring_sizes(mesh, n):
    try:
        coords = [tuple(d.coords) for d in mesh.devices[:, 0]]
        nz = len({c[2] for c in coords})
        nx = len({c[0] for c in coords})
        if nz * nx == n and nz > 1:
            return nz, nx
    except Exception:
        pass
    return n, 1


def attend(mesh, query_proj, projected_keys, projected_values):
    n, ntp = mesh.shape["sp"], mesh.shape["tp"]
    nz, nx = ring_sizes(mesh, n)
    toks, width = query_proj.shape
    heads = width // HEAD_SIZE
    group = heads // (projected_keys.shape[1] // HEAD_SIZE)
    spare = LANES - projected_keys.shape[1]
    if spare:
        projected_keys = jnp.pad(projected_keys, ((0, 0), (0, spare)))
        projected_values = jnp.pad(projected_values, ((0, 0), (0, spare)))
    quarter = HEAD_SIZE // 4
    places = lax.axis_index("sp") * toks + jnp.arange(toks, dtype=jnp.int32)
    frequency = base_theta ** (-jnp.arange(quarter, dtype=jnp.float32) / quarter)
    lane = jnp.arange(LANES, dtype=jnp.int32)
    on_row = (lane % HEAD_SIZE) < 2 * quarter
    spot = jnp.where(on_row[None, :], (places // GRID_W)[:, None], (places % GRID_W)[:, None])
    angle = spot.astype(jnp.float32) * jnp.tile(frequency, LANES // quarter)[None, :]
    first = (lane // quarter) % 2 == 0
    source = jnp.where(first, lane + quarter, lane - quarter)
    swap = jnp.where(
        lane[:, None] == source[None, :], jnp.where(first, -1.0, 1.0)[None, :], 0.0
    ).astype(jnp.bfloat16)
    ones = jnp.where(
        lane[:, None] // HEAD_SIZE == lane[None, :] // HEAD_SIZE, 1.0 / HEAD_SIZE, 0.0
    ).astype(jnp.bfloat16)
    share = toks // ntp
    dma = pltpu.SemaphoreType.DMA
    return pl.pallas_call(
        functools.partial(attend_kernel, n, nz, nx, ntp, group),
        out_shape=jax.ShapeDtypeStruct((share, ntp * width), jnp.bfloat16),
        in_specs=[pl.BlockSpec(memory_space=pltpu.VMEM)] * 7,
        out_specs=pl.BlockSpec(memory_space=pltpu.VMEM),
        scratch_shapes=[
            pltpu.VMEM((heads * toks, LANES), jnp.bfloat16),
            pltpu.VMEM((heads * toks, LANES), jnp.float32),
            pltpu.VMEM((n + 1, 2, toks // 2, LANES), jnp.bfloat16),
            pltpu.VMEM((n + 1, 2, toks // 2, LANES), jnp.bfloat16),
            pltpu.VMEM((ntp, share, width), jnp.bfloat16),
            pltpu.VMEM((ntp, share, width), jnp.bfloat16),
            dma((n - 1,)), dma((n - 1,)), dma((n - 1,)), dma((n - 1,)),
            dma((ntp,)), dma((ntp,)),
        ],
        compiler_params=pltpu.CompilerParams(
            collective_id=0, has_side_effects=True, vmem_limit_bytes=40 << 20
        ),
        name="attend",
    )(query_proj, projected_keys, projected_values, jnp.cos(angle), jnp.sin(angle), swap, ones)


def moe_kernel(
    nz, nx, ntp, cap, cuts, pieces,
    normed, stream, route, share_w, gate_hbm, up_hbm, down_hbm,
    out_ref,
    info, blk, tx, rx, res, ret, inc, part, snd, place, weigh, act, gate, up, down,
    send_i, recv_i, send_u, send_d, recv_z, send_o, recv_o, send_r, recv_r, send_p, recv_p, wsem,
):
    sp = lax.axis_index("sp")
    tp = lax.axis_index("tp")
    z = sp // nx
    p = (sp % nx) * ntp + tp
    plane = nx * ntp
    slots = plane * cap
    toks, width = normed.shape
    wide = width // cuts
    fine = width // pieces
    others = (plane - 1) * cap

    def device(zz, pp):
        return (zz * nx + pp // ntp, pp % ntp)

    peers = [(p + q) % plane for q in range(plane)]
    homes = [device(z, pp) for pp in peers]

    def cols(c):
        return pl.ds(pl.multiple_of(c * wide, wide), wide)

    def part_cols(c):
        return pl.ds(pl.multiple_of(c * fine, fine), fine)

    def rows(pp):
        return pl.ds(pl.multiple_of(pp * cap, cap), cap)

    def remote(src, dst, send, recv, to):
        return pltpu.make_async_remote_copy(
            src_ref=src, dst_ref=dst, send_sem=send, recv_sem=recv,
            device_id=to, device_id_type=MESH,
        )

    def loop(first, last, action):
        def body(i, carry):
            action(i)
            return carry

        lax.fori_loop(first, last, body, 0)

    def facts(k):
        to = (z + k) % nz
        return remote(info.at[z], info.at[z], send_i.at[k], recv_i.at[k], device(to, p))

    def facts_in(k):
        zz = (z - k + nz) % nz
        return remote(info.at[zz], info.at[zz], send_i.at[k], recv_i.at[k], device(zz, p))

    def own_hop(c, up_way):
        send = send_u if up_way else send_d
        return remote(
            normed.at[:, cols(c)], blk.at[z, :, cols(c)], send.at[z, c], recv_z.at[z, c],
            device(z + 1 if up_way else z - 1, p),
        )

    def hop(zz, c, up_way):
        send = send_u if up_way else send_d
        return remote(
            blk.at[zz, :, cols(c)], blk.at[zz, :, cols(c)], send.at[zz, c], recv_z.at[zz, c],
            device(z + 1 if up_way else z - 1, p),
        )

    def dispatch(zz, c, q):
        pp = peers[q]
        return remote(
            tx.at[zz, rows(pp), cols(c)], rx.at[zz, rows(p), cols(c)],
            send_o.at[zz], recv_o.at[zz], homes[q],
        )

    def dispatch_all(zz):
        some = pl.ds(0, others)
        return remote(tx.at[zz, some], rx.at[zz, some], send_o.at[zz], recv_o.at[zz], device(z, p))

    def answer(zz, c, q):
        pp = peers[q]
        return remote(
            res.at[zz, rows(pp), part_cols(c)], ret.at[zz, rows(p), part_cols(c)],
            send_r.at[zz], recv_r.at[zz, c], homes[q],
        )

    def answer_in(zz, c):
        some = pl.ds(0, others)
        return remote(
            res.at[zz, some, part_cols(c)], ret.at[zz, some, part_cols(c)],
            send_r.at[zz], recv_r.at[zz, c], device(z, p),
        )

    def answer_sent(zz):
        some = pl.ds(0, others)
        return remote(res.at[zz, some], ret.at[zz, some], send_r.at[zz], recv_r.at[zz, 0], device(z, p))

    def starts(zz):
        return jnp.where(zz > z, z == 0, z == nz - 1)

    def partial_out(zz, c):
        slot = jnp.where(zz == z + 1, nz, zz)
        return remote(
            snd.at[zz, :, part_cols(c)], inc.at[slot, :, part_cols(c)],
            send_p.at[zz, c], recv_p.at[slot, c], device(z + jnp.where(zz > z, 1, -1), p),
        )

    def partial_in(slot, c):
        return remote(
            snd.at[0, :, part_cols(c)], inc.at[slot, :, part_cols(c)],
            send_p.at[0, c], recv_p.at[slot, c], device(z, p),
        )

    barrier = pltpu.get_barrier_semaphore()
    for k in range(1, nz):
        pl.semaphore_signal(barrier, inc=1, device_id=device((z + k) % nz, p), device_id_type=MESH)
    for q in range(1, plane):
        pl.semaphore_signal(barrier, inc=1, device_id=device(z, (p + q) % plane), device_id_type=MESH)
    loads = [
        pltpu.make_async_copy(gate_hbm.at[0], gate, wsem.at[0]),
        pltpu.make_async_copy(up_hbm.at[0], up, wsem.at[1]),
        pltpu.make_async_copy(down_hbm.at[0], down, wsem.at[2]),
    ]
    for load in loads:
        load.start()

    experts = nz * plane
    at_expert = lax.broadcasted_iota(jnp.int32, (experts, toks), 0)
    named = [at_expert == route[k : k + 1, :] for k in range(2)]
    count = (named[0].astype(jnp.float32) + named[1].astype(jnp.float32)).astype(jnp.bfloat16)
    before = (
        lax.broadcasted_iota(jnp.int32, (toks, toks), 0)
        < lax.broadcasted_iota(jnp.int32, (toks, toks), 1)
    ).astype(jnp.float32).astype(jnp.bfloat16)
    earlier = jnp.dot(count, before, preferred_element_type=jnp.float32)
    lines = []
    for k in range(2):
        rank = jnp.sum(jnp.where(named[k], earlier, 0.0), axis=0, keepdims=True)
        lines.append(route[k : k + 1, :].astype(jnp.float32) * float(cap) + rank)
    info[z] = jnp.concatenate(
        lines + [share_w[...], jnp.zeros((4, toks), jnp.float32)], axis=0
    )

    pl.semaphore_wait(barrier, nz - 1 + plane - 1)
    for k in range(1, nz):
        facts(k).start()

    @pl.when(z + 1 < nz)
    def _():
        loop(0, cuts, lambda c: own_hop(c, True).start())

    @pl.when(z > 0)
    def _():
        loop(0, cuts, lambda c: own_hop(c, False).start())

    def learn(zz):
        known = info[zz]
        spot = (
            lax.broadcasted_iota(jnp.int32, (slots, toks), 0) + z * slots
        ).astype(jnp.float32)
        first = spot == known[0:1, :]
        second = spot == known[1:2, :]
        place[zz] = jnp.where(first | second, 1.0, 0.0).astype(jnp.bfloat16)
        amount = jnp.where(first, known[2:3, :], 0.0) + jnp.where(second, known[3:4, :], 0.0)
        turned = amount.T
        hi = turned.astype(jnp.bfloat16)
        weigh[zz, :, 0:slots] = hi
        weigh[zz, :, slots : 2 * slots] = (turned - hi.astype(jnp.float32)).astype(jnp.bfloat16)

    def pack(zz, c, block):
        packed = jnp.dot(
            place[zz], block, preferred_element_type=jnp.float32
        ).astype(jnp.bfloat16)
        tx[zz, :, cols(c)] = packed
        for q in range(1, plane):
            dispatch(zz, c, q).start()
        rx[zz, rows(p), cols(c)] = tx[zz, rows(p), cols(c)]

    def columns(first, total, most, body):
        tile = math.gcd(total, most)

        def one(c, carry):
            body(pl.ds(pl.multiple_of(first + c * tile, tile), tile))
            return carry

        lax.fori_loop(0, total // tile, one, 0)

    def expert(zz):
        dispatch_all(zz).wait_recv()

        def hidden(at):
            taken = rx[zz]
            pre = jnp.dot(taken, gate[:, at], preferred_element_type=jnp.float32)
            lift = jnp.dot(taken, up[:, at], preferred_element_type=jnp.float32)
            act[:, at] = (pre / (1.0 + jnp.exp(-pre)) * lift).astype(jnp.bfloat16)

        def project(at):
            res[zz, :, at] = jnp.dot(
                act[...], down[:, at], preferred_element_type=jnp.float32
            ).astype(jnp.bfloat16)

        columns(0, gate.shape[1], max(256, min(1024, 131072 // slots)), hidden)

        def send(c):
            columns(c * fine, fine, 512, project)
            for q in range(1, plane):
                answer(zz, c, q).start()
            ret[zz, rows(p), part_cols(c)] = res[zz, rows(p), part_cols(c)]

        loop(0, pieces, send)

    def gather(zz, c):
        answer_in(zz, c).wait_recv()
        back = ret[zz, :, part_cols(c)]
        total = jnp.dot(
            weigh[zz, :, 0:slots], back, preferred_element_type=jnp.float32
        ) + jnp.dot(
            weigh[zz, :, slots : 2 * slots], back, preferred_element_type=jnp.float32
        )
        part[zz, :, part_cols(c)] = total

        @pl.when(jnp.logical_and(zz != z, starts(zz)))
        def _():
            snd[zz, :, part_cols(c)] = total.astype(jnp.bfloat16)
            partial_out(zz, c).start()

    def both(d, action):
        def side(s, carry):
            zz = z + d * (2 * s - 1)
            valid = jnp.logical_and(jnp.logical_and(zz >= 0, zz < nz), jnp.logical_or(d > 0, s == 0))

            @pl.when(valid)
            def _():
                action(zz, s)

            return carry

        lax.fori_loop(0, 2, side, 0)

    def receive(d, c):
        def forward(zz, s):
            hop(zz, c, True).wait_recv()

            @pl.when(jnp.logical_and(zz < z, z + 1 < nz))
            def _():
                hop(zz, c, True).start()

            @pl.when(jnp.logical_and(zz > z, z > 0))
            def _():
                hop(zz, c, False).start()

        both(d, forward)
        both(d, lambda zz, s: pack(zz, c, blk[zz, :, cols(c)]))

    learn(z)
    loop(0, cuts, lambda c: pack(z, c, normed[:, cols(c)]))
    for k in range(1, nz):
        facts_in(k).wait_recv()
        learn((z - k + nz) % nz)
    for load in loads:
        load.wait()

    below = 2 * z < nz - 1
    inner = jnp.logical_and(z > 0, z < nz - 1)

    def relay(level, step, lag):
        def pass_on(s, carry):
            upward = jnp.where(below, s == 0, s == 1)
            zz = jnp.where(upward, level, nz - 1 - level)
            c = step - s * lag
            valid = jnp.logical_and(
                jnp.where(upward, zz > z, zz < z), jnp.logical_not(starts(zz))
            )
            valid = jnp.logical_and(valid, jnp.logical_and(c >= 0, c < pieces))

            @pl.when(valid)
            def _():
                partial_in(zz, c).wait_recv()
                snd[zz, :, part_cols(c)] = (
                    part[zz, :, part_cols(c)] + inc[zz, :, part_cols(c)].astype(jnp.float32)
                ).astype(jnp.bfloat16)
                partial_out(zz, c).start()

            return carry

        lax.fori_loop(0, 2, pass_on, 0)

    def turn(d, carry):
        @pl.when(d < nz)
        def _():
            receive(d, 0)

        both(d - 1, lambda zz, s: expert(zz))

        @pl.when(d < nz)
        def _():
            loop(1, cuts, lambda c: receive(d, c))

        def collect(c):
            @pl.when(jnp.logical_and(d == nz - 1, inner))
            def _():
                loop(1, nz - 1, lambda level: relay(level, c, 0))

            @pl.when(d > 1)
            def _():
                both(d - 1, lambda zz, s: gather(zz, c))

        loop(0, pieces, collect)
        return carry

    lax.fori_loop(1, nz + 1, turn, 0)
    loop(0, pieces, lambda c: gather(z, c))
    loop(0, pieces + 2, lambda c: relay(nz - 1, c, 2))

    def finish(c):
        for slot, there in ((nz, z > 0), (z, z + 1 < nz)):

            @pl.when(there)
            def _():
                partial_in(slot, c).wait_recv()
                part[z, :, part_cols(c)] += inc[slot, :, part_cols(c)].astype(jnp.float32)

        out_ref[:, part_cols(c)] = (
            stream[:, part_cols(c)].astype(jnp.float32) + part[z, :, part_cols(c)]
        ).astype(jnp.bfloat16)

    loop(0, pieces, finish)

    for k in range(1, nz):
        facts(k).wait_send()

    def sent(zz):
        dispatch_all(zz).wait_send()
        answer_sent(zz).wait_send()

        def one(c):
            @pl.when(jnp.logical_and(zz <= z, z + 1 < nz))
            def _():
                hop(zz, c, True).wait_send()

            @pl.when(jnp.logical_and(zz >= z, z > 0))
            def _():
                hop(zz, c, False).wait_send()

        def returned(c):
            @pl.when(zz != z)
            def _():
                partial_out(zz, c).wait_send()

        loop(0, cuts, one)
        loop(0, pieces, returned)

    loop(0, nz, sent)


def moe(mesh, nz, nx, cap, normed, stream, route, share_w, expert_gate, expert_up, expert_down):
    ntp = mesh.shape["tp"]
    plane = nx * ntp
    slots = plane * cap
    toks, width = normed.shape
    ff = expert_gate.shape[2]
    cuts = max(1, width // 1024)
    pieces = max(1, width // 512)
    dma = pltpu.SemaphoreType.DMA
    low = jnp.bfloat16
    return pl.pallas_call(
        functools.partial(moe_kernel, nz, nx, ntp, cap, cuts, pieces),
        out_shape=jax.ShapeDtypeStruct(stream.shape, low),
        in_specs=[pl.BlockSpec(memory_space=pltpu.VMEM)] * 4
        + [pl.BlockSpec(memory_space=pl.ANY)] * 3,
        out_specs=pl.BlockSpec(memory_space=pltpu.VMEM),
        scratch_shapes=[
            pltpu.VMEM((nz, 8, toks), jnp.float32),
            pltpu.VMEM((nz, toks, width), low),
            pltpu.VMEM((nz, slots, width), low),
            pltpu.VMEM((nz, slots, width), low),
            pltpu.VMEM((nz, slots, width), low),
            pltpu.VMEM((nz, slots, width), low),
            pltpu.VMEM((nz + 1, toks, width), low),
            pltpu.VMEM((nz, toks, width), jnp.float32),
            pltpu.VMEM((nz, toks, width), low),
            pltpu.VMEM((nz, slots, toks), low),
            pltpu.VMEM((nz, toks, 2 * slots), low),
            pltpu.VMEM((slots, ff), low),
            pltpu.VMEM((width, ff), low),
            pltpu.VMEM((width, ff), low),
            pltpu.VMEM((ff, width), low),
            dma((nz,)), dma((nz,)),
            dma((nz, cuts)), dma((nz, cuts)), dma((nz, cuts)),
            dma((nz,)), dma((nz,)),
            dma((nz,)), dma((nz, pieces)),
            dma((nz, pieces)), dma((nz + 1, pieces)),
            dma((3,)),
        ],
        compiler_params=pltpu.CompilerParams(
            collective_id=1, has_side_effects=True, vmem_limit_bytes=62 << 20
        ),
        name="moe",
    )(normed, stream, route, share_w, expert_gate, expert_up, expert_down)


def local(
    mesh,
    query_proj,
    projected_keys,
    projected_values,
    residual,
    out_weight,
    mix_gain,
    norm_gain,
    route_expert,
    route_weight,
    expert_gate,
    expert_up,
    expert_down,
):
    by_token = attend(mesh, query_proj, projected_keys, projected_values)
    mixed = jnp.dot(by_token, out_weight, preferred_element_type=jnp.float32)
    stream = (residual.astype(jnp.float32) + unit_length_rows(mixed) * mix_gain).astype(
        jnp.bfloat16
    )
    normed = (unit_length_rows(stream) * norm_gain).astype(jnp.bfloat16)
    row_count = normed.shape[0]
    top_count = route_expert.shape[1]
    n = mesh.shape["sp"]
    experts = n * mesh.shape["tp"]
    capacity = -(-max(2, 2 * top_count * row_count // experts) // 16) * 16
    nz, nx = ring_sizes(mesh, n)
    return moe(
        mesh, nz, nx, capacity, normed, stream, route_expert.T, route_weight.T,
        expert_gate, expert_up, expert_down,
    )


def solution(mesh):
    return jax.shard_map(
        functools.partial(local, mesh),
        mesh=mesh,
        in_specs=(
            P("sp", "tp"),
            P("sp", "tp"),
            P("sp", "tp"),
            P(("sp", "tp"), None),
            P(),
            P(),
            P(),
            P(("sp", "tp"), None),
            P(("sp", "tp"), None),
            P(("sp", "tp"), None, None),
            P(("sp", "tp"), None, None),
            P(("sp", "tp"), None, None),
        ),
        out_specs=P(("sp", "tp"), None),
        check_vma=False,
    )
```

```python
import functools
import math

import jax
import jax.numpy as jnp
from jax import lax
from jax.experimental import pallas as pl
from jax.experimental.pallas import tpu as pltpu
from jax.sharding import PartitionSpec as P

D = 2048
HEAD_SIZE = 64
GRID_W = 64


epsilon = 1e-06
base_theta = 10000.0


def unit_length_rows(values):
    values = values.astype(jnp.float32)
    return values * lax.rsqrt(jnp.mean(values * values, axis=-1, keepdims=True) + epsilon)


MESH = pl.DeviceIdType.MESH
LANES = 2 * HEAD_SIZE


def ring_step(sp, delta, n, nz, nx):
    z, x = sp // nx, sp % nx
    place = x * nz + z + (x % 2) * (nz - 1 - 2 * z)
    place = (place + delta + n) % n
    x = place // nz
    z = place % nz
    z = z + (x % 2) * (nz - 1 - 2 * z)
    return z * nx + x


def attend_kernel(
    n, nz, nx, ntp, group,
    q_ref, k_ref, v_ref, cos_ref, sin_ref,
    out_ref,
    qs, acc, fb, bb, att, rx,
    send_f, recv_f, send_b, recv_b, send_t, recv_t,
    fused=None,
):
    sp = lax.axis_index("sp")
    tp = lax.axis_index("tp")
    toks = q_ref.shape[0]
    heads = q_ref.shape[1] // HEAD_SIZE
    half = toks // 2
    steps = n - 1
    nxt = ring_step(sp, 1, n, nz, nx)
    prv = ring_step(sp, -1, n, nz, nx)

    barrier = pltpu.get_barrier_semaphore()
    for other in (nxt, prv):
        pl.semaphore_signal(barrier, inc=1, device_id=(other, tp), device_id_type=MESH)
    for d in range(1, ntp):
        pl.semaphore_signal(
            barrier, inc=1, device_id=(sp, (tp + d) % ntp), device_id_type=MESH
        )

    lane = lax.broadcasted_iota(jnp.int32, (LANES, LANES), 1)
    other = lax.broadcasted_iota(jnp.int32, (LANES, LANES), 0)
    quarter = HEAD_SIZE // 4
    first = (lane // quarter) % 2 == 0
    swap = jnp.where(
        other == jnp.where(first, lane + quarter, lane - quarter),
        jnp.where(first, -1.0, 1.0), 0.0,
    ).astype(jnp.bfloat16)
    ones = jnp.where(
        other // HEAD_SIZE == lane // HEAD_SIZE, 1.0 / HEAD_SIZE, 0.0
    ).astype(jnp.bfloat16)
    span = math.gcd(toks, GRID_W)
    on_row = lax.broadcasted_iota(jnp.int32, (span, LANES), 1) % HEAD_SIZE < 2 * quarter

    def spread(table):
        columns = table[0:span]
        return jnp.concatenate(
            [
                jnp.where(on_row, table[span + i : span + i + 1], columns)
                for i in range(toks // span)
            ],
            axis=0,
        )

    cos = spread(cos_ref)
    sin = spread(sin_ref)
    low = lax.broadcasted_iota(jnp.int32, (toks, LANES), 1) < HEAD_SIZE

    def prepare(block):
        wide = block.astype(jnp.float32)
        square = wide * wide
        hi = square.astype(jnp.bfloat16)
        lo = (square - hi.astype(jnp.float32)).astype(jnp.bfloat16)
        mean = jnp.dot(hi, ones, preferred_element_type=jnp.float32) + jnp.dot(
            lo, ones, preferred_element_type=jnp.float32
        )
        partner = jnp.dot(block, swap, preferred_element_type=jnp.float32)
        return (wide * cos + partner * sin) * lax.rsqrt(mean + epsilon)

    awaited = 2 + ntp - 1
    if fused is not None:
        awaited += fused["greet"]()
        fused["inputs"](0)
    keys = prepare(k_ref[...]).astype(jnp.bfloat16)
    vals = v_ref[...]
    for c in range(2):
        rows = slice(c * half, (c + 1) * half)
        fb[c, 0] = keys[rows]
        fb[c, 1] = vals[rows]
        bb[1 - c, 0] = keys[rows]
        bb[1 - c, 1] = vals[rows]

    def forward(i):
        return pltpu.make_async_remote_copy(
            src_ref=fb.at[i], dst_ref=fb.at[i + 2],
            send_sem=send_f.at[i], recv_sem=recv_f.at[i],
            device_id=(nxt, tp), device_id_type=MESH,
        )

    def backward(i):
        return pltpu.make_async_remote_copy(
            src_ref=bb.at[i], dst_ref=bb.at[i + 2],
            send_sem=send_b.at[i], recv_sem=recv_b.at[i],
            device_id=(prv, tp), device_id_type=MESH,
        )

    pl.semaphore_wait(barrier, awaited)
    if fused is not None:
        fused["share"]()
    for i in range(2):
        forward(i).start()
        backward(i).start()

    if fused is not None:
        fused["inputs"](1)
    scale = HEAD_SIZE ** (-0.5)
    for t in range(heads // 2):
        ready = prepare(q_ref[:, t * LANES : (t + 1) * LANES]) * scale
        for h in (2 * t, 2 * t + 1):
            side = (h // group) % 2
            lined = ready if h % 2 == side else pltpu.roll(ready, HEAD_SIZE, 1)
            keep = low if side == 0 else jnp.logical_not(low)
            qs[h * toks : (h + 1) * toks] = jnp.where(keep, lined, 0.0).astype(jnp.bfloat16)
    acc[...] = jnp.zeros_like(acc)
    tile = math.gcd(toks, 256)
    vlow = lax.broadcasted_iota(jnp.int32, (toks, LANES), 1) < HEAD_SIZE

    def one_step(j, carry):
        at = j + jnp.minimum(j, 1)

        @pl.when(j > 0)
        def _():
            forward(j - 1).wait_recv()
            backward(j - 1).wait_recv()

        @pl.when(jnp.logical_and(j > 0, j + 1 < steps))
        def _():
            forward(j + 1).start()
            backward(j + 1).start()

        kk = jnp.concatenate([fb[at, 0], bb[at, 0]], axis=0)
        vv = jnp.concatenate([fb[at, 1], bb[at, 1]], axis=0).astype(jnp.float32)
        sided = (
            jnp.where(vlow, vv, 1.0).astype(jnp.bfloat16),
            jnp.where(vlow, 1.0, vv).astype(jnp.bfloat16),
        )
        for h in range(heads):
            for r in range(toks // tile):
                rows = slice(h * toks + r * tile, h * toks + (r + 1) * tile)
                scores = lax.dot_general(
                    qs[rows], kk, (((1,), (1,)), ((), ())),
                    preferred_element_type=jnp.float32,
                )
                weights = jnp.exp(scores).astype(jnp.bfloat16)
                acc[rows] += jnp.dot(
                    weights, sided[(h // group) % 2], preferred_element_type=jnp.float32
                )
        return carry

    if fused is not None:
        fused["learn"]()
    lax.fori_loop(0, steps + 1, one_step, 0)

    share = toks // ntp
    for t in range(heads // 2):
        parts = []
        for h in (2 * t, 2 * t + 1):
            mine = acc[h * toks : (h + 1) * toks]
            turned = pltpu.roll(mine, HEAD_SIZE, 1)
            parts.append(mine / turned if h % 2 == (h // group) % 2 else turned / mine)
        done = jnp.where(low, parts[0], parts[1]).astype(jnp.bfloat16)
        for p in range(ntp):
            att[p, :, t * LANES : (t + 1) * LANES] = done[p * share : (p + 1) * share]

    def across(d):
        to = (tp + d) % ntp
        return pltpu.make_async_remote_copy(
            src_ref=att.at[to], dst_ref=rx.at[tp],
            send_sem=send_t.at[d], recv_sem=recv_t.at[d],
            device_id=(sp, to), device_id_type=MESH,
        )

    for d in range(1, ntp):
        across(d).start()
    if fused is not None:
        fused["mix"](tp, att.at[tp], True)
        for d in range(1, ntp):
            source = (tp + ntp - d) % ntp
            across(d).wait_recv()
            fused["mix"](source, rx.at[source], False)
        fused["norm"]()
    else:
        rx[tp] = att[tp]
        for d in range(1, ntp):
            across(d).wait_recv()
        width = q_ref.shape[1]
        for p in range(ntp):
            out_ref[:, p * width : (p + 1) * width] = rx[p]
    for i in range(steps):
        forward(i).wait_send()
        backward(i).wait_send()
    for d in range(1, ntp):
        across(d).wait_send()


def ring_sizes(mesh, n):
    try:
        coords = [tuple(d.coords) for d in mesh.devices[:, 0]]
        nz = len({c[2] for c in coords})
        nx = len({c[0] for c in coords})
        if nz * nx == n and nz > 1:
            return nz, nx
    except Exception:
        pass
    return n, 1


def attend_inputs(query_proj, projected_keys, projected_values):
    toks, width = query_proj.shape
    heads = width // HEAD_SIZE
    group = heads // (projected_keys.shape[1] // HEAD_SIZE)
    spare = LANES - projected_keys.shape[1]
    if spare:
        projected_keys = jnp.pad(projected_keys, ((0, 0), (0, spare)))
        projected_values = jnp.pad(projected_values, ((0, 0), (0, spare)))
    quarter = HEAD_SIZE // 4
    span = math.gcd(toks, GRID_W)
    places = lax.axis_index("sp") * toks
    frequency = base_theta ** (-jnp.arange(quarter, dtype=jnp.float32) / quarter)
    starts = places + span * jnp.arange(toks // span, dtype=jnp.int32)
    spot = jnp.concatenate(
        [(places % GRID_W) + jnp.arange(span, dtype=jnp.int32), starts // GRID_W]
    )
    angle = spot.astype(jnp.float32)[:, None] * jnp.tile(frequency, LANES // quarter)[None, :]
    return group, projected_keys, projected_values, (jnp.cos(angle), jnp.sin(angle))


def attend(mesh, nz, nx, query_proj, projected_keys, projected_values):
    n, ntp = mesh.shape["sp"], mesh.shape["tp"]
    toks, width = query_proj.shape
    group, projected_keys, projected_values, tables = attend_inputs(
        query_proj, projected_keys, projected_values
    )
    return pl.pallas_call(
        functools.partial(attend_kernel, n, nz, nx, ntp, group),
        out_shape=jax.ShapeDtypeStruct((toks // ntp, ntp * width), jnp.bfloat16),
        in_specs=[pl.BlockSpec(memory_space=pltpu.VMEM)] * 5,
        out_specs=pl.BlockSpec(memory_space=pltpu.VMEM),
        scratch_shapes=attend_scratch(n, ntp, toks, width),
        compiler_params=pltpu.CompilerParams(
            collective_id=0, has_side_effects=True, vmem_limit_bytes=40 << 20
        ),
        name="attend",
    )(query_proj, projected_keys, projected_values, *tables)


def moe_steps(
    nz, nx, ntp, cap, cuts, pieces,
    normed, stream, route, share_w, gate_hbm, up_hbm, down_hbm,
    out_ref,
    info, blk, tx, rx, res, ret, inc, part, snd, place, weigh, act, gate, up, down,
    send_i, recv_i, send_u, send_d, recv_z, send_o, recv_o, send_r, recv_r, send_p, recv_p, wsem,
):
    sp = lax.axis_index("sp")
    tp = lax.axis_index("tp")
    z = sp // nx
    p = (sp % nx) * ntp + tp
    plane = nx * ntp
    slots = plane * cap
    toks, width = normed.shape
    wide = width // cuts
    fine = width // pieces
    others = (plane - 1) * cap

    def device(zz, pp):
        return (zz * nx + pp // ntp, pp % ntp)

    peers = [(p + q) % plane for q in range(plane)]
    homes = [device(z, pp) for pp in peers]

    def cols(c):
        return pl.ds(pl.multiple_of(c * wide, wide), wide)

    def part_cols(c):
        return pl.ds(pl.multiple_of(c * fine, fine), fine)

    def rows(pp):
        return pl.ds(pl.multiple_of(pp * cap, cap), cap)

    def remote(src, dst, send, recv, to):
        return pltpu.make_async_remote_copy(
            src_ref=src, dst_ref=dst, send_sem=send, recv_sem=recv,
            device_id=to, device_id_type=MESH,
        )

    def loop(first, last, action):
        def body(i, carry):
            action(i)
            return carry

        lax.fori_loop(first, last, body, 0)

    def facts(k):
        to = (z + k) % nz
        return remote(info.at[z], info.at[z], send_i.at[k], recv_i.at[k], device(to, p))

    def facts_in(k):
        zz = (z - k + nz) % nz
        return remote(info.at[zz], info.at[zz], send_i.at[k], recv_i.at[k], device(zz, p))

    def own_hop(c, up_way):
        send = send_u if up_way else send_d
        return remote(
            normed.at[:, cols(c)], blk.at[z, :, cols(c)], send.at[z, c], recv_z.at[z, c],
            device(z + 1 if up_way else z - 1, p),
        )

    def hop(zz, c, up_way):
        send = send_u if up_way else send_d
        return remote(
            blk.at[zz, :, cols(c)], blk.at[zz, :, cols(c)], send.at[zz, c], recv_z.at[zz, c],
            device(z + 1 if up_way else z - 1, p),
        )

    def dispatch(zz, c, q):
        pp = peers[q]
        return remote(
            tx.at[zz, rows(pp), cols(c)], rx.at[zz, rows(p), cols(c)],
            send_o.at[zz], recv_o.at[zz], homes[q],
        )

    def dispatch_all(zz):
        some = pl.ds(0, others)
        return remote(tx.at[zz, some], rx.at[zz, some], send_o.at[zz], recv_o.at[zz], device(z, p))

    def answer(zz, c, q):
        pp = peers[q]
        return remote(
            res.at[zz, rows(pp), part_cols(c)], ret.at[zz, rows(p), part_cols(c)],
            send_r.at[zz], recv_r.at[zz, c], homes[q],
        )

    def answer_in(zz, c):
        some = pl.ds(0, others)
        return remote(
            res.at[zz, some, part_cols(c)], ret.at[zz, some, part_cols(c)],
            send_r.at[zz], recv_r.at[zz, c], device(z, p),
        )

    def answer_sent(zz):
        some = pl.ds(0, others)
        return remote(res.at[zz, some], ret.at[zz, some], send_r.at[zz], recv_r.at[zz, 0], device(z, p))

    def starts(zz):
        return jnp.where(zz > z, z == 0, z == nz - 1)

    def partial_out(zz, c):
        slot = jnp.where(zz == z + 1, nz, zz)
        return remote(
            snd.at[zz, :, part_cols(c)], inc.at[slot, :, part_cols(c)],
            send_p.at[zz, c], recv_p.at[slot, c], device(z + jnp.where(zz > z, 1, -1), p),
        )

    def partial_in(slot, c):
        return remote(
            snd.at[0, :, part_cols(c)], inc.at[slot, :, part_cols(c)],
            send_p.at[0, c], recv_p.at[slot, c], device(z, p),
        )

    loads = [
        pltpu.make_async_copy(gate_hbm.at[0], gate, wsem.at[0]),
        pltpu.make_async_copy(up_hbm.at[0], up, wsem.at[1]),
        pltpu.make_async_copy(down_hbm.at[0], down, wsem.at[2]),
    ]

    def greet():
        barrier = pltpu.get_barrier_semaphore()
        for k in range(1, nz):
            pl.semaphore_signal(
                barrier, inc=1, device_id=device((z + k) % nz, p), device_id_type=MESH
            )
        for q in range(1, plane):
            pl.semaphore_signal(barrier, inc=1, device_id=homes[q], device_id_type=MESH)
        return nz - 1 + plane - 1

    def fetch():
        for load in loads:
            load.start()

    def own_facts():
        experts = nz * plane
        at_expert = lax.broadcasted_iota(jnp.int32, (experts, toks), 0)
        named = [at_expert == route[k : k + 1, :] for k in range(2)]
        count = (named[0].astype(jnp.float32) + named[1].astype(jnp.float32)).astype(jnp.bfloat16)
        before = (
            lax.broadcasted_iota(jnp.int32, (toks, toks), 0)
            < lax.broadcasted_iota(jnp.int32, (toks, toks), 1)
        ).astype(jnp.float32).astype(jnp.bfloat16)
        earlier = jnp.dot(count, before, preferred_element_type=jnp.float32)
        lines = []
        for k in range(2):
            rank = jnp.sum(jnp.where(named[k], earlier, 0.0), axis=0, keepdims=True)
            lines.append(route[k : k + 1, :].astype(jnp.float32) * float(cap) + rank)
        info[z] = jnp.concatenate(
            lines + [share_w[...], jnp.zeros((4, toks), jnp.float32)], axis=0
        )

    def share_facts():
        for k in range(1, nz):
            facts(k).start()

    def send_own(c):
        @pl.when(z + 1 < nz)
        def _():
            own_hop(c, True).start()

        @pl.when(z > 0)
        def _():
            own_hop(c, False).start()

    def learn(zz):
        known = info[zz]
        spot = (
            lax.broadcasted_iota(jnp.int32, (slots, toks), 0) + z * slots
        ).astype(jnp.float32)
        first = spot == known[0:1, :]
        second = spot == known[1:2, :]
        place[zz] = jnp.where(first | second, 1.0, 0.0).astype(jnp.bfloat16)
        amount = jnp.where(first, known[2:3, :], 0.0) + jnp.where(second, known[3:4, :], 0.0)
        turned = amount.T
        hi = turned.astype(jnp.bfloat16)
        weigh[zz, :, 0:slots] = hi
        weigh[zz, :, slots : 2 * slots] = (turned - hi.astype(jnp.float32)).astype(jnp.bfloat16)

    def pack(zz, c, block):
        packed = jnp.dot(
            place[zz], block, preferred_element_type=jnp.float32
        ).astype(jnp.bfloat16)
        tx[zz, :, cols(c)] = packed
        for q in range(1, plane):
            dispatch(zz, c, q).start()
        rx[zz, rows(p), cols(c)] = tx[zz, rows(p), cols(c)]

    def columns(first, total, most, body):
        tile = math.gcd(total, most)

        def one(c, carry):
            body(pl.ds(pl.multiple_of(first + c * tile, tile), tile))
            return carry

        lax.fori_loop(0, total // tile, one, 0)

    def expert(zz):
        dispatch_all(zz).wait_recv()

        def hidden(at):
            taken = rx[zz]
            pre = jnp.dot(taken, gate[:, at], preferred_element_type=jnp.float32)
            lift = jnp.dot(taken, up[:, at], preferred_element_type=jnp.float32)
            act[:, at] = (pre / (1.0 + jnp.exp(-pre)) * lift).astype(jnp.bfloat16)

        def project(at):
            res[zz, :, at] = jnp.dot(
                act[...], down[:, at], preferred_element_type=jnp.float32
            ).astype(jnp.bfloat16)

        columns(0, gate.shape[1], max(256, min(1024, 131072 // slots)), hidden)

        def send(c):
            columns(c * fine, fine, 512, project)
            for q in range(1, plane):
                answer(zz, c, q).start()
            ret[zz, rows(p), part_cols(c)] = res[zz, rows(p), part_cols(c)]

        loop(0, pieces, send)

    def gather(zz, c):
        answer_in(zz, c).wait_recv()
        back = ret[zz, :, part_cols(c)]
        total = jnp.dot(
            weigh[zz, :, 0:slots], back, preferred_element_type=jnp.float32
        ) + jnp.dot(
            weigh[zz, :, slots : 2 * slots], back, preferred_element_type=jnp.float32
        )
        part[zz, :, part_cols(c)] = total

        @pl.when(jnp.logical_and(zz != z, starts(zz)))
        def _():
            snd[zz, :, part_cols(c)] = total.astype(jnp.bfloat16)
            partial_out(zz, c).start()

    def both(d, action):
        def side(s, carry):
            zz = z + d * (2 * s - 1)
            valid = jnp.logical_and(jnp.logical_and(zz >= 0, zz < nz), jnp.logical_or(d > 0, s == 0))

            @pl.when(valid)
            def _():
                action(zz, s)

            return carry

        lax.fori_loop(0, 2, side, 0)

    def receive(d, c):
        def forward(zz, s):
            hop(zz, c, True).wait_recv()

            @pl.when(jnp.logical_and(zz < z, z + 1 < nz))
            def _():
                hop(zz, c, True).start()

            @pl.when(jnp.logical_and(zz > z, z > 0))
            def _():
                hop(zz, c, False).start()

        both(d, forward)
        both(d, lambda zz, s: pack(zz, c, blk[zz, :, cols(c)]))

    def learn_others():
        for k in range(1, nz):
            facts_in(k).wait_recv()
            learn((z - k + nz) % nz)

    def pack_own(c):
        pack(z, c, normed[:, cols(c)])

    below = 2 * z < nz - 1
    inner = jnp.logical_and(z > 0, z < nz - 1)

    def relay(level, step, lag):
        def pass_on(s, carry):
            upward = jnp.where(below, s == 0, s == 1)
            zz = jnp.where(upward, level, nz - 1 - level)
            c = step - s * lag
            valid = jnp.logical_and(
                jnp.where(upward, zz > z, zz < z), jnp.logical_not(starts(zz))
            )
            valid = jnp.logical_and(valid, jnp.logical_and(c >= 0, c < pieces))

            @pl.when(valid)
            def _():
                partial_in(zz, c).wait_recv()
                snd[zz, :, part_cols(c)] = (
                    part[zz, :, part_cols(c)] + inc[zz, :, part_cols(c)].astype(jnp.float32)
                ).astype(jnp.bfloat16)
                partial_out(zz, c).start()

            return carry

        lax.fori_loop(0, 2, pass_on, 0)

    def turn(d, carry):
        @pl.when(d < nz)
        def _():
            receive(d, 0)

        @pl.when(jnp.logical_or(inner, d > 1))
        def _():
            both(d - 1, lambda zz, s: expert(zz))

        @pl.when(d < nz)
        def _():
            loop(1, cuts, lambda c: receive(d, c))

        @pl.when(jnp.logical_and(d == nz, jnp.logical_not(inner)))
        def _():
            expert(z)

        def collect(c):
            @pl.when(jnp.logical_and(d == nz - 1, inner))
            def _():
                loop(1, nz - 1, lambda level: relay(level, c, 0))

            @pl.when(d > 1)
            def _():
                both(d - 1, lambda zz, s: gather(zz, c))

        loop(0, pieces, collect)

        return carry

    def finish(c):
        for slot, there in ((nz, z > 0), (z, z + 1 < nz)):

            @pl.when(there)
            def _():
                partial_in(slot, c).wait_recv()
                part[z, :, part_cols(c)] += inc[slot, :, part_cols(c)].astype(jnp.float32)

        out_ref[:, part_cols(c)] = (
            stream[:, part_cols(c)].astype(jnp.float32) + part[z, :, part_cols(c)]
        ).astype(jnp.bfloat16)

    def sent(zz):
        dispatch_all(zz).wait_send()
        answer_sent(zz).wait_send()

        def one(c):
            @pl.when(jnp.logical_and(zz <= z, z + 1 < nz))
            def _():
                hop(zz, c, True).wait_send()

            @pl.when(jnp.logical_and(zz >= z, z > 0))
            def _():
                hop(zz, c, False).wait_send()

        def returned(c):
            @pl.when(zz != z)
            def _():
                partial_out(zz, c).wait_send()

        loop(0, cuts, one)
        loop(0, pieces, returned)

    def run():
        for load in loads:
            load.wait()
        lax.fori_loop(1, nz + 1, turn, 0)
        loop(0, pieces, lambda c: gather(z, c))
        loop(0, pieces + 2, lambda c: relay(nz - 1, c, 2))
        loop(0, pieces, finish)

        for k in range(1, nz):
            facts(k).wait_send()
        loop(0, nz, sent)

    return dict(
        greet=greet, fetch=fetch, own_facts=own_facts, share_facts=share_facts, learn=learn,
        learn_others=learn_others, send_own=send_own, pack_own=pack_own, run=run, place=z,
    )


def moe_kernel(nz, nx, ntp, cap, cuts, pieces, *refs):
    steps = moe_steps(nz, nx, ntp, cap, cuts, pieces, *refs)
    awaited = steps["greet"]()
    steps["fetch"]()
    steps["own_facts"]()
    pl.semaphore_wait(pltpu.get_barrier_semaphore(), awaited)
    steps["share_facts"]()
    for c in range(cuts):
        steps["send_own"](c)
    steps["learn"](steps["place"])
    for c in range(cuts):
        steps["pack_own"](c)
    steps["learn_others"]()
    steps["run"]()


def layer_kernel(n, nz, nx, ntp, group, cap, cuts, pieces, parts, *refs):
    (
        q_hbm, k_hbm, v_hbm, residual_hbm, mixer_hbm, cos, sin,
        mix_gain, norm_gain, route, share_w, gate_hbm, up_hbm, down_hbm, out_ref,
        q, k, v, residual, mixer, normed, stream, insem,
    ) = refs[:23]
    attend_refs = refs[23 : 23 + parts]
    moe_refs = refs[23 + parts :]
    mixed = moe_refs[7].at[0]
    copies = [
        pltpu.make_async_copy(src, dst, insem.at[i])
        for i, (src, dst) in enumerate(
            ((k_hbm, k), (v_hbm, v), (q_hbm, q), (residual_hbm, residual), (mixer_hbm, mixer))
        )
    ]
    for copy in copies:
        copy.start()
    steps = moe_steps(
        nz, nx, ntp, cap, cuts, pieces,
        normed, stream, route, share_w, gate_hbm, up_hbm, down_hbm, out_ref, *moe_refs,
    )

    def inputs(stage):
        for copy in copies[:2] if stage == 0 else copies[2:3]:
            copy.wait()

    def greet():
        awaited = steps["greet"]()
        steps["fetch"]()
        steps["own_facts"]()
        return awaited

    def learn():
        steps["learn"](steps["place"])
        steps["learn_others"]()

    toks, width = normed.shape
    depth = q.shape[1]
    tile = width // cuts

    def each(action):
        for c in range(cuts):
            action(c, slice(c * tile, (c + 1) * tile))

    def mix(source, block, first):
        if first:
            for copy in copies[3:]:
                copy.wait()
        rows = pl.ds(pl.multiple_of(source * depth, depth), depth)

        def one(c, at):
            term = jnp.dot(block[...], mixer[rows, at], preferred_element_type=jnp.float32)
            mixed[:, at] = term if first else mixed[:, at] + term

        each(one)

    def norm():
        def squares(values):
            return jnp.sum(values * values, axis=-1, keepdims=True)

        total = jnp.zeros((toks, 1), jnp.float32)
        for c in range(cuts):
            total += squares(mixed[:, c * tile : (c + 1) * tile])
        scale = lax.rsqrt(total / width + epsilon)
        total = jnp.zeros((toks, 1), jnp.float32)
        for c in range(cuts):
            at = slice(c * tile, (c + 1) * tile)
            row = (
                residual[:, at].astype(jnp.float32) + mixed[:, at] * scale * mix_gain[:, at]
            ).astype(jnp.bfloat16)
            stream[:, at] = row
            total += squares(row.astype(jnp.float32))
        scale = lax.rsqrt(total / width + epsilon)
        for c in range(cuts):
            at = slice(c * tile, (c + 1) * tile)
            normed[:, at] = (
                stream[:, at].astype(jnp.float32) * scale * norm_gain[:, at]
            ).astype(jnp.bfloat16)
            steps["send_own"](c)
        for c in range(cuts):
            steps["pack_own"](c)

    attend_kernel(
        n, nz, nx, ntp, group, q, k, v, cos, sin, None, *attend_refs,
        fused=dict(
            greet=greet, inputs=inputs, share=steps["share_facts"], learn=learn, mix=mix, norm=norm
        ),
    )
    steps["run"]()


def attend_scratch(n, ntp, toks, width):
    heads = width // HEAD_SIZE
    share = toks // ntp
    dma = pltpu.SemaphoreType.DMA
    return [
        pltpu.VMEM((heads * toks, LANES), jnp.bfloat16),
        pltpu.VMEM((heads * toks, LANES), jnp.float32),
        pltpu.VMEM((n + 1, 2, toks // 2, LANES), jnp.bfloat16),
        pltpu.VMEM((n + 1, 2, toks // 2, LANES), jnp.bfloat16),
        pltpu.VMEM((ntp, share, width), jnp.bfloat16),
        pltpu.VMEM((ntp, share, width), jnp.bfloat16),
        dma((n - 1,)), dma((n - 1,)), dma((n - 1,)), dma((n - 1,)),
        dma((ntp,)), dma((ntp,)),
    ]


def moe_scratch(nz, slots, toks, width, ff, cuts, pieces):
    dma = pltpu.SemaphoreType.DMA
    low = jnp.bfloat16
    return [
        pltpu.VMEM((nz, 8, toks), jnp.float32),
        pltpu.VMEM((nz, toks, width), low),
        pltpu.VMEM((nz, slots, width), low),
        pltpu.VMEM((nz, slots, width), low),
        pltpu.VMEM((nz, slots, width), low),
        pltpu.VMEM((nz, slots, width), low),
        pltpu.VMEM((nz + 1, toks, width), low),
        pltpu.VMEM((nz, toks, width), jnp.float32),
        pltpu.VMEM((nz, toks, width), low),
        pltpu.VMEM((nz, slots, toks), low),
        pltpu.VMEM((nz, toks, 2 * slots), low),
        pltpu.VMEM((slots, ff), low),
        pltpu.VMEM((width, ff), low),
        pltpu.VMEM((width, ff), low),
        pltpu.VMEM((ff, width), low),
        dma((nz,)), dma((nz,)),
        dma((nz, cuts)), dma((nz, cuts)), dma((nz, cuts)),
        dma((nz,)), dma((nz,)),
        dma((nz,)), dma((nz, pieces)),
        dma((nz, pieces)), dma((nz + 1, pieces)),
        dma((3,)),
    ]


def moe(mesh, nz, nx, cap, normed, stream, route, share_w, expert_gate, expert_up, expert_down):
    ntp = mesh.shape["tp"]
    slots = nx * ntp * cap
    toks, width = normed.shape
    ff = expert_gate.shape[2]
    cuts = max(1, width // 1024)
    pieces = max(1, width // 512)
    return pl.pallas_call(
        functools.partial(moe_kernel, nz, nx, ntp, cap, cuts, pieces),
        out_shape=jax.ShapeDtypeStruct(stream.shape, jnp.bfloat16),
        in_specs=[pl.BlockSpec(memory_space=pltpu.VMEM)] * 4
        + [pl.BlockSpec(memory_space=pl.ANY)] * 3,
        out_specs=pl.BlockSpec(memory_space=pltpu.VMEM),
        scratch_shapes=moe_scratch(nz, slots, toks, width, ff, cuts, pieces),
        compiler_params=pltpu.CompilerParams(
            collective_id=1, has_side_effects=True, vmem_limit_bytes=62 << 20
        ),
        name="moe",
    )(normed, stream, route, share_w, expert_gate, expert_up, expert_down)


def layer(
    mesh, nz, nx, cap, query_proj, projected_keys, projected_values, residual, out_weight,
    mix_gain, norm_gain, route, share_w, expert_gate, expert_up, expert_down,
):
    n, ntp = mesh.shape["sp"], mesh.shape["tp"]
    slots = nx * ntp * cap
    group, projected_keys, projected_values, tables = attend_inputs(
        query_proj, projected_keys, projected_values
    )
    toks, depth = query_proj.shape
    rows, width = residual.shape
    ff = expert_gate.shape[2]
    cuts = max(1, width // 1024)
    pieces = max(1, width // 512)
    low = jnp.bfloat16
    inner = attend_scratch(n, ntp, toks, depth)
    vmem = pl.BlockSpec(memory_space=pltpu.VMEM)
    anywhere = pl.BlockSpec(memory_space=pl.ANY)
    return pl.pallas_call(
        functools.partial(
            layer_kernel, n, nz, nx, ntp, group, cap, cuts, pieces, len(inner)
        ),
        out_shape=jax.ShapeDtypeStruct(residual.shape, low),
        in_specs=[anywhere] * 5 + [vmem] * 6 + [anywhere] * 3,
        out_specs=vmem,
        scratch_shapes=[
            pltpu.VMEM((toks, depth), low),
            pltpu.VMEM(projected_keys.shape, low),
            pltpu.VMEM(projected_values.shape, low),
            pltpu.VMEM((rows, width), low),
            pltpu.VMEM(out_weight.shape, low),
            pltpu.VMEM((rows, width), low),
            pltpu.VMEM((rows, width), low),
            pltpu.SemaphoreType.DMA((5,)),
        ]
        + inner
        + moe_scratch(nz, slots, rows, width, ff, cuts, pieces),
        compiler_params=pltpu.CompilerParams(
            collective_id=2, has_side_effects=True, vmem_limit_bytes=62 << 20
        ),
        name="layer",
    )(
        query_proj, projected_keys, projected_values, residual, out_weight, *tables,
        mix_gain[None, :], norm_gain[None, :], route, share_w,
        expert_gate, expert_up, expert_down,
    )


def local(
    mesh,
    query_proj,
    projected_keys,
    projected_values,
    residual,
    out_weight,
    mix_gain,
    norm_gain,
    route_expert,
    route_weight,
    expert_gate,
    expert_up,
    expert_down,
):
    row_count = residual.shape[0]
    top_count = route_expert.shape[1]
    n, ntp = mesh.shape["sp"], mesh.shape["tp"]
    experts = n * ntp
    capacity = -(-max(2, 2 * top_count * row_count // experts) // 16) * 16
    nz, nx = ring_sizes(mesh, n)
    if nx * ntp * capacity <= 128:
        return layer(
            mesh, nz, nx, capacity, query_proj, projected_keys, projected_values, residual,
            out_weight, mix_gain, norm_gain, route_expert.T, route_weight.T,
            expert_gate, expert_up, expert_down,
        )
    by_token = attend(mesh, nz, nx, query_proj, projected_keys, projected_values)
    mixed = jnp.dot(by_token, out_weight, preferred_element_type=jnp.float32)
    stream = (residual.astype(jnp.float32) + unit_length_rows(mixed) * mix_gain).astype(
        jnp.bfloat16
    )
    normed = (unit_length_rows(stream) * norm_gain).astype(jnp.bfloat16)
    return moe(
        mesh, nz, nx, capacity, normed, stream, route_expert.T, route_weight.T,
        expert_gate, expert_up, expert_down,
    )


def solution(mesh):
    return jax.shard_map(
        functools.partial(local, mesh),
        mesh=mesh,
        in_specs=(
            P("sp", "tp"),
            P("sp", "tp"),
            P("sp", "tp"),
            P(("sp", "tp"), None),
            P(),
            P(),
            P(),
            P(("sp", "tp"), None),
            P(("sp", "tp"), None),
            P(("sp", "tp"), None, None),
            P(("sp", "tp"), None, None),
            P(("sp", "tp"), None, None),
        ),
        out_specs=P(("sp", "tp"), None),
        check_vma=False,
    )
```

```python
import functools
import math

import jax
import jax.numpy as jnp
from jax import lax
from jax.experimental import pallas as pl
from jax.experimental.pallas import tpu as pltpu
from jax.sharding import PartitionSpec as P

D = 2048
HEAD_SIZE = 64
GRID_W = 64


epsilon = 1e-06
base_theta = 10000.0


def unit_length_rows(values):
    values = values.astype(jnp.float32)
    return values * lax.rsqrt(jnp.mean(values * values, axis=-1, keepdims=True) + epsilon)


MESH = pl.DeviceIdType.MESH
LANES = 2 * HEAD_SIZE


def ring_step(sp, delta, n, nz, nx):
    z, x = sp // nx, sp % nx
    place = x * nz + z + (x % 2) * (nz - 1 - 2 * z)
    place = (place + delta + n) % n
    x = place // nz
    z = place % nz
    z = z + (x % 2) * (nz - 1 - 2 * z)
    return z * nx + x


def attend_kernel(
    n, nz, nx, ntp, group,
    q_ref, k_ref, v_ref, cos_ref, sin_ref,
    out_ref,
    qs, acc, fb, bb, att, rx,
    send_f, recv_f, send_b, recv_b, send_t, recv_t,
    fused=None,
):
    sp = lax.axis_index("sp")
    tp = lax.axis_index("tp")
    toks = q_ref.shape[0]
    heads = q_ref.shape[1] // HEAD_SIZE
    half = toks // 2
    steps = n - 1
    nxt = ring_step(sp, 1, n, nz, nx)
    prv = ring_step(sp, -1, n, nz, nx)

    barrier = pltpu.get_barrier_semaphore()
    for other in (nxt, prv):
        pl.semaphore_signal(barrier, inc=1, device_id=(other, tp), device_id_type=MESH)
    for d in range(1, ntp):
        pl.semaphore_signal(
            barrier, inc=1, device_id=(sp, (tp + d) % ntp), device_id_type=MESH
        )

    lane = lax.broadcasted_iota(jnp.int32, (LANES, LANES), 1)
    other = lax.broadcasted_iota(jnp.int32, (LANES, LANES), 0)
    quarter = HEAD_SIZE // 4
    first = (lane // quarter) % 2 == 0
    swap = jnp.where(
        other == jnp.where(first, lane + quarter, lane - quarter),
        jnp.where(first, -1.0, 1.0), 0.0,
    ).astype(jnp.bfloat16)
    ones = jnp.where(
        other // HEAD_SIZE == lane // HEAD_SIZE, 1.0 / HEAD_SIZE, 0.0
    ).astype(jnp.bfloat16)
    span = math.gcd(toks, GRID_W)
    on_row = lax.broadcasted_iota(jnp.int32, (span, LANES), 1) % HEAD_SIZE < 2 * quarter

    def spread(table):
        columns = table[0:span]
        return jnp.concatenate(
            [
                jnp.where(on_row, table[span + i : span + i + 1], columns)
                for i in range(toks // span)
            ],
            axis=0,
        )

    cos = spread(cos_ref)
    sin = spread(sin_ref)
    low = lax.broadcasted_iota(jnp.int32, (toks, LANES), 1) < HEAD_SIZE

    def prepare(block):
        wide = block.astype(jnp.float32)
        square = wide * wide
        hi = square.astype(jnp.bfloat16)
        lo = (square - hi.astype(jnp.float32)).astype(jnp.bfloat16)
        mean = jnp.dot(hi, ones, preferred_element_type=jnp.float32) + jnp.dot(
            lo, ones, preferred_element_type=jnp.float32
        )
        partner = jnp.dot(block, swap, preferred_element_type=jnp.float32)
        return (wide * cos + partner * sin) * lax.rsqrt(mean + epsilon)

    awaited = 2 + ntp - 1
    if fused is not None:
        awaited += fused["greet"]()
        fused["inputs"](0)
    keys = prepare(k_ref[...]).astype(jnp.bfloat16)
    vals = v_ref[...]
    for c in range(2):
        rows = slice(c * half, (c + 1) * half)
        fb[c, 0] = keys[rows]
        fb[c, 1] = vals[rows]
        bb[1 - c, 0] = keys[rows]
        bb[1 - c, 1] = vals[rows]

    def forward(i):
        return pltpu.make_async_remote_copy(
            src_ref=fb.at[i], dst_ref=fb.at[i + 2],
            send_sem=send_f.at[i], recv_sem=recv_f.at[i],
            device_id=(nxt, tp), device_id_type=MESH,
        )

    def backward(i):
        return pltpu.make_async_remote_copy(
            src_ref=bb.at[i], dst_ref=bb.at[i + 2],
            send_sem=send_b.at[i], recv_sem=recv_b.at[i],
            device_id=(prv, tp), device_id_type=MESH,
        )

    pl.semaphore_wait(barrier, awaited)
    if fused is not None:
        fused["share"]()
    for i in range(2):
        forward(i).start()
        backward(i).start()

    if fused is not None:
        fused["inputs"](1)
    scale = HEAD_SIZE ** (-0.5)
    for t in range(heads // 2):
        ready = prepare(q_ref[:, t * LANES : (t + 1) * LANES]) * scale
        for h in (2 * t, 2 * t + 1):
            side = (h // group) % 2
            lined = ready if h % 2 == side else pltpu.roll(ready, HEAD_SIZE, 1)
            keep = low if side == 0 else jnp.logical_not(low)
            qs[h * toks : (h + 1) * toks] = jnp.where(keep, lined, 0.0).astype(jnp.bfloat16)
    acc[...] = jnp.zeros_like(acc)
    tile = math.gcd(toks, 256)
    vlow = lax.broadcasted_iota(jnp.int32, (toks, LANES), 1) < HEAD_SIZE

    def one_step(j, carry):
        at = j + jnp.minimum(j, 1)

        @pl.when(j > 0)
        def _():
            forward(j - 1).wait_recv()
            backward(j - 1).wait_recv()

        @pl.when(jnp.logical_and(j > 0, j + 1 < steps))
        def _():
            forward(j + 1).start()
            backward(j + 1).start()

        kk = jnp.concatenate([fb[at, 0], bb[at, 0]], axis=0)
        vv = jnp.concatenate([fb[at, 1], bb[at, 1]], axis=0).astype(jnp.float32)
        sided = (
            jnp.where(vlow, vv, 1.0).astype(jnp.bfloat16),
            jnp.where(vlow, 1.0, vv).astype(jnp.bfloat16),
        )
        for h in range(heads):
            for r in range(toks // tile):
                rows = slice(h * toks + r * tile, h * toks + (r + 1) * tile)
                scores = lax.dot_general(
                    qs[rows], kk, (((1,), (1,)), ((), ())),
                    preferred_element_type=jnp.float32,
                )
                weights = jnp.exp(scores).astype(jnp.bfloat16)
                acc[rows] += jnp.dot(
                    weights, sided[(h // group) % 2], preferred_element_type=jnp.float32
                )
        return carry

    if fused is not None:
        fused["learn"]()
    lax.fori_loop(0, steps + 1, one_step, 0)

    share = toks // ntp
    for t in range(heads // 2):
        parts = []
        for h in (2 * t, 2 * t + 1):
            mine = acc[h * toks : (h + 1) * toks]
            turned = pltpu.roll(mine, HEAD_SIZE, 1)
            parts.append(mine / turned if h % 2 == (h // group) % 2 else turned / mine)
        done = jnp.where(low, parts[0], parts[1]).astype(jnp.bfloat16)
        for p in range(ntp):
            att[p, :, t * LANES : (t + 1) * LANES] = done[p * share : (p + 1) * share]

    def across(d):
        to = (tp + d) % ntp
        return pltpu.make_async_remote_copy(
            src_ref=att.at[to], dst_ref=rx.at[tp],
            send_sem=send_t.at[d], recv_sem=recv_t.at[d],
            device_id=(sp, to), device_id_type=MESH,
        )

    for d in range(1, ntp):
        across(d).start()
    if fused is not None:
        fused["mix"](tp, att.at[tp], True)
        for d in range(1, ntp):
            source = (tp + ntp - d) % ntp
            across(d).wait_recv()
            fused["mix"](source, rx.at[source], False)
        fused["norm"]()
    else:
        rx[tp] = att[tp]
        for d in range(1, ntp):
            across(d).wait_recv()
        width = q_ref.shape[1]
        for p in range(ntp):
            out_ref[:, p * width : (p + 1) * width] = rx[p]
    for i in range(steps):
        forward(i).wait_send()
        backward(i).wait_send()
    for d in range(1, ntp):
        across(d).wait_send()


def ring_sizes(mesh, n):
    try:
        coords = [tuple(d.coords) for d in mesh.devices[:, 0]]
        nz = len({c[2] for c in coords})
        nx = len({c[0] for c in coords})
        if nz * nx == n and nz > 1:
            return nz, nx
    except Exception:
        pass
    return n, 1


def attend_inputs(query_proj, projected_keys, projected_values):
    toks, width = query_proj.shape
    heads = width // HEAD_SIZE
    group = heads // (projected_keys.shape[1] // HEAD_SIZE)
    spare = LANES - projected_keys.shape[1]
    if spare:
        projected_keys = jnp.pad(projected_keys, ((0, 0), (0, spare)))
        projected_values = jnp.pad(projected_values, ((0, 0), (0, spare)))
    quarter = HEAD_SIZE // 4
    span = math.gcd(toks, GRID_W)
    places = lax.axis_index("sp") * toks
    frequency = base_theta ** (-jnp.arange(quarter, dtype=jnp.float32) / quarter)
    starts = places + span * jnp.arange(toks // span, dtype=jnp.int32)
    spot = jnp.concatenate(
        [(places % GRID_W) + jnp.arange(span, dtype=jnp.int32), starts // GRID_W]
    )
    angle = spot.astype(jnp.float32)[:, None] * jnp.tile(frequency, LANES // quarter)[None, :]
    return group, projected_keys, projected_values, (jnp.cos(angle), jnp.sin(angle))


def attend(mesh, nz, nx, query_proj, projected_keys, projected_values):
    n, ntp = mesh.shape["sp"], mesh.shape["tp"]
    toks, width = query_proj.shape
    group, projected_keys, projected_values, tables = attend_inputs(
        query_proj, projected_keys, projected_values
    )
    return pl.pallas_call(
        functools.partial(attend_kernel, n, nz, nx, ntp, group),
        out_shape=jax.ShapeDtypeStruct((toks // ntp, ntp * width), jnp.bfloat16),
        in_specs=[pl.BlockSpec(memory_space=pltpu.VMEM)] * 5,
        out_specs=pl.BlockSpec(memory_space=pltpu.VMEM),
        scratch_shapes=attend_scratch(n, ntp, toks, width),
        compiler_params=pltpu.CompilerParams(
            collective_id=0, has_side_effects=True, vmem_limit_bytes=40 << 20
        ),
        name="attend",
    )(query_proj, projected_keys, projected_values, *tables)


def moe_steps(
    nz, nx, ntp, cap, cuts, pieces,
    normed, stream, route, share_w, gate_hbm, up_hbm, down_hbm,
    out_ref,
    info, blk, tx, rx, res, ret, inc, part, snd, place, weigh, act, gate, up, down,
    send_i, recv_i, send_u, send_d, recv_z, send_o, recv_o, send_r, recv_r, send_p, recv_p, wsem,
):
    sp = lax.axis_index("sp")
    tp = lax.axis_index("tp")
    z = sp // nx
    p = (sp % nx) * ntp + tp
    plane = nx * ntp
    slots = plane * cap
    toks, width = normed.shape
    wide = width // cuts
    fine = width // pieces
    others = (plane - 1) * cap

    def device(zz, pp):
        return (zz * nx + pp // ntp, pp % ntp)

    peers = [(p + q) % plane for q in range(plane)]
    homes = [device(z, pp) for pp in peers]

    def cols(c):
        return pl.ds(pl.multiple_of(c * wide, wide), wide)

    def part_cols(c):
        return pl.ds(pl.multiple_of(c * fine, fine), fine)

    def rows(pp):
        return pl.ds(pl.multiple_of(pp * cap, cap), cap)

    def remote(src, dst, send, recv, to):
        return pltpu.make_async_remote_copy(
            src_ref=src, dst_ref=dst, send_sem=send, recv_sem=recv,
            device_id=to, device_id_type=MESH,
        )

    def loop(first, last, action):
        def body(i, carry):
            action(i)
            return carry

        lax.fori_loop(first, last, body, 0)

    def facts(k):
        to = (z + k) % nz
        return remote(info.at[z], info.at[z], send_i.at[k], recv_i.at[k], device(to, p))

    def facts_in(k):
        zz = (z - k + nz) % nz
        return remote(info.at[zz], info.at[zz], send_i.at[k], recv_i.at[k], device(zz, p))

    def own_hop(c, up_way):
        send = send_u if up_way else send_d
        return remote(
            normed.at[:, cols(c)], blk.at[z, :, cols(c)], send.at[z, c], recv_z.at[z, c],
            device(z + 1 if up_way else z - 1, p),
        )

    def hop(zz, c, up_way):
        send = send_u if up_way else send_d
        return remote(
            blk.at[zz, :, cols(c)], blk.at[zz, :, cols(c)], send.at[zz, c], recv_z.at[zz, c],
            device(z + 1 if up_way else z - 1, p),
        )

    def dispatch(zz, c, q):
        pp = peers[q]
        return remote(
            tx.at[zz, rows(pp), cols(c)], rx.at[zz, rows(p), cols(c)],
            send_o.at[zz], recv_o.at[zz], homes[q],
        )

    def dispatch_all(zz):
        some = pl.ds(0, others)
        return remote(tx.at[zz, some], rx.at[zz, some], send_o.at[zz], recv_o.at[zz], device(z, p))

    def answer(zz, c, q):
        pp = peers[q]
        return remote(
            res.at[zz, rows(pp), part_cols(c)], ret.at[zz, rows(p), part_cols(c)],
            send_r.at[zz], recv_r.at[zz, c], homes[q],
        )

    def answer_in(zz, c):
        some = pl.ds(0, others)
        return remote(
            res.at[zz, some, part_cols(c)], ret.at[zz, some, part_cols(c)],
            send_r.at[zz], recv_r.at[zz, c], device(z, p),
        )

    def answer_sent(zz):
        some = pl.ds(0, others)
        return remote(res.at[zz, some], ret.at[zz, some], send_r.at[zz], recv_r.at[zz, 0], device(z, p))

    def starts(zz):
        return jnp.where(zz > z, z == 0, z == nz - 1)

    def partial_out(zz, c):
        slot = jnp.where(zz == z + 1, nz, zz)
        return remote(
            snd.at[zz, :, part_cols(c)], inc.at[slot, :, part_cols(c)],
            send_p.at[zz, c], recv_p.at[slot, c], device(z + jnp.where(zz > z, 1, -1), p),
        )

    def partial_in(slot, c):
        return remote(
            snd.at[0, :, part_cols(c)], inc.at[slot, :, part_cols(c)],
            send_p.at[0, c], recv_p.at[slot, c], device(z, p),
        )

    loads = [
        pltpu.make_async_copy(gate_hbm.at[0], gate, wsem.at[0]),
        pltpu.make_async_copy(up_hbm.at[0], up, wsem.at[1]),
        pltpu.make_async_copy(down_hbm.at[0], down, wsem.at[2]),
    ]

    def greet():
        barrier = pltpu.get_barrier_semaphore()
        for k in range(1, nz):
            pl.semaphore_signal(
                barrier, inc=1, device_id=device((z + k) % nz, p), device_id_type=MESH
            )
        for q in range(1, plane):
            pl.semaphore_signal(barrier, inc=1, device_id=homes[q], device_id_type=MESH)
        return nz - 1 + plane - 1

    def fetch():
        for load in loads:
            load.start()

    def own_facts():
        experts = nz * plane
        at_expert = lax.broadcasted_iota(jnp.int32, (experts, toks), 0)
        named = [at_expert == route[k : k + 1, :] for k in range(2)]
        count = (named[0].astype(jnp.float32) + named[1].astype(jnp.float32)).astype(jnp.bfloat16)
        before = (
            lax.broadcasted_iota(jnp.int32, (toks, toks), 0)
            < lax.broadcasted_iota(jnp.int32, (toks, toks), 1)
        ).astype(jnp.float32).astype(jnp.bfloat16)
        earlier = jnp.dot(count, before, preferred_element_type=jnp.float32)
        lines = []
        for k in range(2):
            rank = jnp.sum(jnp.where(named[k], earlier, 0.0), axis=0, keepdims=True)
            lines.append(route[k : k + 1, :].astype(jnp.float32) * float(cap) + rank)
        info[z] = jnp.concatenate(
            lines + [share_w[...], jnp.zeros((4, toks), jnp.float32)], axis=0
        )

    def share_facts():
        for k in range(1, nz):
            facts(k).start()

    def send_own(c):
        @pl.when(z + 1 < nz)
        def _():
            own_hop(c, True).start()

        @pl.when(z > 0)
        def _():
            own_hop(c, False).start()

    def learn(zz):
        known = info[zz]
        spot = (
            lax.broadcasted_iota(jnp.int32, (slots, toks), 0) + z * slots
        ).astype(jnp.float32)
        first = spot == known[0:1, :]
        second = spot == known[1:2, :]
        place[zz] = jnp.where(first | second, 1.0, 0.0).astype(jnp.bfloat16)
        amount = jnp.where(first, known[2:3, :], 0.0) + jnp.where(second, known[3:4, :], 0.0)
        turned = amount.T
        hi = turned.astype(jnp.bfloat16)
        weigh[zz, :, 0:slots] = hi
        weigh[zz, :, slots : 2 * slots] = (turned - hi.astype(jnp.float32)).astype(jnp.bfloat16)

    def pack(zz, c, block):
        packed = jnp.dot(
            place[zz], block, preferred_element_type=jnp.float32
        ).astype(jnp.bfloat16)
        tx[zz, :, cols(c)] = packed
        for q in range(1, plane):
            dispatch(zz, c, q).start()
        rx[zz, rows(p), cols(c)] = tx[zz, rows(p), cols(c)]

    def columns(first, total, most, body):
        tile = math.gcd(total, most)

        def one(c, carry):
            body(pl.ds(pl.multiple_of(first + c * tile, tile), tile))
            return carry

        lax.fori_loop(0, total // tile, one, 0)

    def expert(zz):
        dispatch_all(zz).wait_recv()

        def hidden(at):
            taken = rx[zz]
            pre = jnp.dot(taken, gate[:, at], preferred_element_type=jnp.float32)
            lift = jnp.dot(taken, up[:, at], preferred_element_type=jnp.float32)
            act[:, at] = (pre / (1.0 + jnp.exp(-pre)) * lift).astype(jnp.bfloat16)

        def project(at):
            res[zz, :, at] = jnp.dot(
                act[...], down[:, at], preferred_element_type=jnp.float32
            ).astype(jnp.bfloat16)

        columns(0, gate.shape[1], max(256, min(1024, 131072 // slots)), hidden)

        def send(c):
            columns(c * fine, fine, 512, project)
            for q in range(1, plane):
                answer(zz, c, q).start()
            ret[zz, rows(p), part_cols(c)] = res[zz, rows(p), part_cols(c)]

        loop(0, pieces, send)

    def gather(zz, c):
        answer_in(zz, c).wait_recv()
        back = ret[zz, :, part_cols(c)]
        total = jnp.dot(
            weigh[zz, :, 0:slots], back, preferred_element_type=jnp.float32
        ) + jnp.dot(
            weigh[zz, :, slots : 2 * slots], back, preferred_element_type=jnp.float32
        )
        part[zz, :, part_cols(c)] = total

        @pl.when(jnp.logical_and(zz != z, starts(zz)))
        def _():
            snd[zz, :, part_cols(c)] = total.astype(jnp.bfloat16)
            partial_out(zz, c).start()

    def both(d, action):
        def side(s, carry):
            zz = z + d * (2 * s - 1)
            valid = jnp.logical_and(jnp.logical_and(zz >= 0, zz < nz), jnp.logical_or(d > 0, s == 0))

            @pl.when(valid)
            def _():
                action(zz, s)

            return carry

        lax.fori_loop(0, 2, side, 0)

    def receive(d, c):
        def forward(zz, s):
            hop(zz, c, True).wait_recv()

            @pl.when(jnp.logical_and(zz < z, z + 1 < nz))
            def _():
                hop(zz, c, True).start()

            @pl.when(jnp.logical_and(zz > z, z > 0))
            def _():
                hop(zz, c, False).start()

        both(d, forward)
        both(d, lambda zz, s: pack(zz, c, blk[zz, :, cols(c)]))

    def learn_others():
        for k in range(1, nz):
            facts_in(k).wait_recv()
            learn((z - k + nz) % nz)

    def pack_own(c):
        pack(z, c, normed[:, cols(c)])

    below = 2 * z < nz - 1
    inner = jnp.logical_and(z > 0, z < nz - 1)

    def relay(level, step, lag):
        def pass_on(s, carry):
            upward = jnp.where(below, s == 0, s == 1)
            zz = jnp.where(upward, level, nz - 1 - level)
            c = step - s * lag
            valid = jnp.logical_and(
                jnp.where(upward, zz > z, zz < z), jnp.logical_not(starts(zz))
            )
            valid = jnp.logical_and(valid, jnp.logical_and(c >= 0, c < pieces))

            @pl.when(valid)
            def _():
                partial_in(zz, c).wait_recv()
                snd[zz, :, part_cols(c)] = (
                    part[zz, :, part_cols(c)] + inc[zz, :, part_cols(c)].astype(jnp.float32)
                ).astype(jnp.bfloat16)
                partial_out(zz, c).start()

            return carry

        lax.fori_loop(0, 2, pass_on, 0)

    def turn(d, carry):
        @pl.when(d < nz)
        def _():
            receive(d, 0)

        @pl.when(jnp.logical_and(d == nz - 1, inner))
        def _():
            loop(1, nz - 1, lambda level: relay(level, 0, 0))

        @pl.when(jnp.logical_or(inner, d > 1))
        def _():
            both(d - 1, lambda zz, s: expert(zz))

        @pl.when(d < nz)
        def _():
            loop(1, cuts, lambda c: receive(d, c))

        @pl.when(jnp.logical_and(d == nz, jnp.logical_not(inner)))
        def _():
            expert(z)

        def collect(c):
            @pl.when(jnp.logical_and(d == nz - 1, inner))
            def _():
                def ahead(step):
                    loop(1, nz - 1, lambda level: relay(level, step, 0))

                loop(c + 1, c + 2, ahead)

            @pl.when(d > 1)
            def _():
                both(d - 1, lambda zz, s: gather(zz, c))

        loop(0, pieces, collect)

        return carry

    def finish(c):
        for slot, there in ((nz, z > 0), (z, z + 1 < nz)):

            @pl.when(there)
            def _():
                partial_in(slot, c).wait_recv()
                part[z, :, part_cols(c)] += inc[slot, :, part_cols(c)].astype(jnp.float32)

        out_ref[:, part_cols(c)] = (
            stream[:, part_cols(c)].astype(jnp.float32) + part[z, :, part_cols(c)]
        ).astype(jnp.bfloat16)

    def sent(zz):
        dispatch_all(zz).wait_send()
        answer_sent(zz).wait_send()

        def one(c):
            @pl.when(jnp.logical_and(zz <= z, z + 1 < nz))
            def _():
                hop(zz, c, True).wait_send()

            @pl.when(jnp.logical_and(zz >= z, z > 0))
            def _():
                hop(zz, c, False).wait_send()

        def returned(c):
            @pl.when(zz != z)
            def _():
                partial_out(zz, c).wait_send()

        loop(0, cuts, one)
        loop(0, pieces, returned)

    def run():
        for load in loads:
            load.wait()
        lax.fori_loop(1, nz + 1, turn, 0)
        loop(0, pieces, lambda c: gather(z, c))
        loop(0, pieces + 2, lambda c: relay(nz - 1, c, 2))
        loop(0, pieces, finish)

        for k in range(1, nz):
            facts(k).wait_send()
        loop(0, nz, sent)

    return dict(
        greet=greet, fetch=fetch, own_facts=own_facts, share_facts=share_facts, learn=learn,
        learn_others=learn_others, send_own=send_own, pack_own=pack_own, run=run, place=z,
    )


def moe_kernel(nz, nx, ntp, cap, cuts, pieces, *refs):
    steps = moe_steps(nz, nx, ntp, cap, cuts, pieces, *refs)
    awaited = steps["greet"]()
    steps["fetch"]()
    steps["own_facts"]()
    pl.semaphore_wait(pltpu.get_barrier_semaphore(), awaited)
    steps["share_facts"]()
    for c in range(cuts):
        steps["send_own"](c)
    steps["learn"](steps["place"])
    for c in range(cuts):
        steps["pack_own"](c)
    steps["learn_others"]()
    steps["run"]()


def layer_kernel(n, nz, nx, ntp, group, cap, cuts, pieces, parts, *refs):
    (
        q_hbm, k_hbm, v_hbm, residual_hbm, mixer_hbm, cos, sin,
        mix_gain, norm_gain, route, share_w, gate_hbm, up_hbm, down_hbm, out_ref,
        q, k, v, residual, mixer, normed, stream, insem,
    ) = refs[:23]
    attend_refs = refs[23 : 23 + parts]
    moe_refs = refs[23 + parts :]
    mixed = moe_refs[7].at[0]
    copies = [
        pltpu.make_async_copy(src, dst, insem.at[i])
        for i, (src, dst) in enumerate(
            ((k_hbm, k), (v_hbm, v), (q_hbm, q), (residual_hbm, residual), (mixer_hbm, mixer))
        )
    ]
    for copy in copies:
        copy.start()
    steps = moe_steps(
        nz, nx, ntp, cap, cuts, pieces,
        normed, stream, route, share_w, gate_hbm, up_hbm, down_hbm, out_ref, *moe_refs,
    )

    def inputs(stage):
        for copy in copies[:2] if stage == 0 else copies[2:3]:
            copy.wait()

    def greet():
        awaited = steps["greet"]()
        steps["fetch"]()
        steps["own_facts"]()
        return awaited

    def learn():
        steps["learn"](steps["place"])
        steps["learn_others"]()

    toks, width = normed.shape
    depth = q.shape[1]
    tile = width // cuts

    def each(action):
        for c in range(cuts):
            action(c, slice(c * tile, (c + 1) * tile))

    def mix(source, block, first):
        if first:
            for copy in copies[3:]:
                copy.wait()
        rows = pl.ds(pl.multiple_of(source * depth, depth), depth)

        def one(c, at):
            term = jnp.dot(block[...], mixer[rows, at], preferred_element_type=jnp.float32)
            mixed[:, at] = term if first else mixed[:, at] + term

        each(one)

    def norm():
        def squares(values):
            return jnp.sum(values * values, axis=-1, keepdims=True)

        total = jnp.zeros((toks, 1), jnp.float32)
        for c in range(cuts):
            total += squares(mixed[:, c * tile : (c + 1) * tile])
        scale = lax.rsqrt(total / width + epsilon)
        total = jnp.zeros((toks, 1), jnp.float32)
        for c in range(cuts):
            at = slice(c * tile, (c + 1) * tile)
            row = (
                residual[:, at].astype(jnp.float32) + mixed[:, at] * scale * mix_gain[:, at]
            ).astype(jnp.bfloat16)
            stream[:, at] = row
            total += squares(row.astype(jnp.float32))
        scale = lax.rsqrt(total / width + epsilon)
        for c in range(cuts):
            at = slice(c * tile, (c + 1) * tile)
            normed[:, at] = (
                stream[:, at].astype(jnp.float32) * scale * norm_gain[:, at]
            ).astype(jnp.bfloat16)
            steps["send_own"](c)
        for c in range(cuts):
            steps["pack_own"](c)

    attend_kernel(
        n, nz, nx, ntp, group, q, k, v, cos, sin, None, *attend_refs,
        fused=dict(
            greet=greet, inputs=inputs, share=steps["share_facts"], learn=learn, mix=mix, norm=norm
        ),
    )
    steps["run"]()


def attend_scratch(n, ntp, toks, width):
    heads = width // HEAD_SIZE
    share = toks // ntp
    dma = pltpu.SemaphoreType.DMA
    return [
        pltpu.VMEM((heads * toks, LANES), jnp.bfloat16),
        pltpu.VMEM((heads * toks, LANES), jnp.float32),
        pltpu.VMEM((n + 1, 2, toks // 2, LANES), jnp.bfloat16),
        pltpu.VMEM((n + 1, 2, toks // 2, LANES), jnp.bfloat16),
        pltpu.VMEM((ntp, share, width), jnp.bfloat16),
        pltpu.VMEM((ntp, share, width), jnp.bfloat16),
        dma((n - 1,)), dma((n - 1,)), dma((n - 1,)), dma((n - 1,)),
        dma((ntp,)), dma((ntp,)),
    ]


def moe_scratch(nz, slots, toks, width, ff, cuts, pieces):
    dma = pltpu.SemaphoreType.DMA
    low = jnp.bfloat16
    return [
        pltpu.VMEM((nz, 8, toks), jnp.float32),
        pltpu.VMEM((nz, toks, width), low),
        pltpu.VMEM((nz, slots, width), low),
        pltpu.VMEM((nz, slots, width), low),
        pltpu.VMEM((nz, slots, width), low),
        pltpu.VMEM((nz, slots, width), low),
        pltpu.VMEM((nz + 1, toks, width), low),
        pltpu.VMEM((nz, toks, width), jnp.float32),
        pltpu.VMEM((nz, toks, width), low),
        pltpu.VMEM((nz, slots, toks), low),
        pltpu.VMEM((nz, toks, 2 * slots), low),
        pltpu.VMEM((slots, ff), low),
        pltpu.VMEM((width, ff), low),
        pltpu.VMEM((width, ff), low),
        pltpu.VMEM((ff, width), low),
        dma((nz,)), dma((nz,)),
        dma((nz, cuts)), dma((nz, cuts)), dma((nz, cuts)),
        dma((nz,)), dma((nz,)),
        dma((nz,)), dma((nz, pieces)),
        dma((nz, pieces)), dma((nz + 1, pieces)),
        dma((3,)),
    ]


def moe(mesh, nz, nx, cap, normed, stream, route, share_w, expert_gate, expert_up, expert_down):
    ntp = mesh.shape["tp"]
    slots = nx * ntp * cap
    toks, width = normed.shape
    ff = expert_gate.shape[2]
    cuts = max(1, width // 1024)
    pieces = max(1, width // 512)
    return pl.pallas_call(
        functools.partial(moe_kernel, nz, nx, ntp, cap, cuts, pieces),
        out_shape=jax.ShapeDtypeStruct(stream.shape, jnp.bfloat16),
        in_specs=[pl.BlockSpec(memory_space=pltpu.VMEM)] * 4
        + [pl.BlockSpec(memory_space=pl.ANY)] * 3,
        out_specs=pl.BlockSpec(memory_space=pltpu.VMEM),
        scratch_shapes=moe_scratch(nz, slots, toks, width, ff, cuts, pieces),
        compiler_params=pltpu.CompilerParams(
            collective_id=1, has_side_effects=True, vmem_limit_bytes=62 << 20
        ),
        name="moe",
    )(normed, stream, route, share_w, expert_gate, expert_up, expert_down)


def layer(
    mesh, nz, nx, cap, query_proj, projected_keys, projected_values, residual, out_weight,
    mix_gain, norm_gain, route, share_w, expert_gate, expert_up, expert_down,
):
    n, ntp = mesh.shape["sp"], mesh.shape["tp"]
    slots = nx * ntp * cap
    group, projected_keys, projected_values, tables = attend_inputs(
        query_proj, projected_keys, projected_values
    )
    toks, depth = query_proj.shape
    rows, width = residual.shape
    ff = expert_gate.shape[2]
    cuts = max(1, width // 1024)
    pieces = max(1, width // 512)
    low = jnp.bfloat16
    inner = attend_scratch(n, ntp, toks, depth)
    vmem = pl.BlockSpec(memory_space=pltpu.VMEM)
    anywhere = pl.BlockSpec(memory_space=pl.ANY)
    return pl.pallas_call(
        functools.partial(
            layer_kernel, n, nz, nx, ntp, group, cap, cuts, pieces, len(inner)
        ),
        out_shape=jax.ShapeDtypeStruct(residual.shape, low),
        in_specs=[anywhere] * 5 + [vmem] * 6 + [anywhere] * 3,
        out_specs=vmem,
        scratch_shapes=[
            pltpu.VMEM((toks, depth), low),
            pltpu.VMEM(projected_keys.shape, low),
            pltpu.VMEM(projected_values.shape, low),
            pltpu.VMEM((rows, width), low),
            pltpu.VMEM(out_weight.shape, low),
            pltpu.VMEM((rows, width), low),
            pltpu.VMEM((rows, width), low),
            pltpu.SemaphoreType.DMA((5,)),
        ]
        + inner
        + moe_scratch(nz, slots, rows, width, ff, cuts, pieces),
        compiler_params=pltpu.CompilerParams(
            collective_id=2, has_side_effects=True, vmem_limit_bytes=62 << 20
        ),
        name="layer",
    )(
        query_proj, projected_keys, projected_values, residual, out_weight, *tables,
        mix_gain[None, :], norm_gain[None, :], route, share_w,
        expert_gate, expert_up, expert_down,
    )


def local(
    mesh,
    query_proj,
    projected_keys,
    projected_values,
    residual,
    out_weight,
    mix_gain,
    norm_gain,
    route_expert,
    route_weight,
    expert_gate,
    expert_up,
    expert_down,
):
    row_count = residual.shape[0]
    top_count = route_expert.shape[1]
    n, ntp = mesh.shape["sp"], mesh.shape["tp"]
    experts = n * ntp
    capacity = -(-max(2, 2 * top_count * row_count // experts) // 16) * 16
    nz, nx = ring_sizes(mesh, n)
    if nx * ntp * capacity <= 128:
        return layer(
            mesh, nz, nx, capacity, query_proj, projected_keys, projected_values, residual,
            out_weight, mix_gain, norm_gain, route_expert.T, route_weight.T,
            expert_gate, expert_up, expert_down,
        )
    by_token = attend(mesh, nz, nx, query_proj, projected_keys, projected_values)
    mixed = jnp.dot(by_token, out_weight, preferred_element_type=jnp.float32)
    stream = (residual.astype(jnp.float32) + unit_length_rows(mixed) * mix_gain).astype(
        jnp.bfloat16
    )
    normed = (unit_length_rows(stream) * norm_gain).astype(jnp.bfloat16)
    return moe(
        mesh, nz, nx, capacity, normed, stream, route_expert.T, route_weight.T,
        expert_gate, expert_up, expert_down,
    )


def solution(mesh):
    return jax.shard_map(
        functools.partial(local, mesh),
        mesh=mesh,
        in_specs=(
            P("sp", "tp"),
            P("sp", "tp"),
            P("sp", "tp"),
            P(("sp", "tp"), None),
            P(),
            P(),
            P(),
            P(("sp", "tp"), None),
            P(("sp", "tp"), None),
            P(("sp", "tp"), None, None),
            P(("sp", "tp"), None, None),
            P(("sp", "tp"), None, None),
        ),
        out_specs=P(("sp", "tp"), None),
        check_vma=False,
    )
```
